256 devices in a mesh: fs: 32 (over z, y), tp: 8 (over x, core).
Axes of the slice: x: 4, y: 4, z: 8, core: 2. Of those that a mesh axis runs over, the one named last changes fastest.
Arguments:
- tokens: bfloat16 [16384, 2048], P('fs', 'tp'), may hold values from -6 to 6
- mixer_gain: float32 [2048], replicated, may hold values from 0.1 to 1.9
- recur_in: bfloat16 [2048, 1024], P('fs', 'tp'), may hold values from -0.125 to 0.125
- branch_in: bfloat16 [2048, 1024], P('fs', 'tp'), may hold values from -0.125 to 0.125
- conv_taps: bfloat16 [4, 1024], replicated, may hold values from -3 to 3
- recur_gate: bfloat16 [2, 16, 64, 64], replicated, may hold values from -0.75 to 0.75
- input_gate: bfloat16 [2, 16, 64, 64], replicated, may hold values from -0.75 to 0.75
- decay_param: float32 [2, 1024], replicated, may hold values from 3.5 to 11
- recur_gain: float32 [1024], replicated, may hold values from 0.1 to 1.9
- recur_out: bfloat16 [1024, 2048], P('tp', 'fs'), may hold values from -0.1875 to 0.1875
- mixer_post: float32 [2048], replicated, may hold values from 0.1 to 1.9
- channel_gain: float32 [2048], replicated, may hold values from 0.1 to 1.9
- hidden_gate: bfloat16 [2048, 5632], P('fs', 'tp'), may hold values from -0.125 to 0.125
- hidden_up: bfloat16 [2048, 5632], P('fs', 'tp'), may hold values from -0.125 to 0.125
- hidden_down: bfloat16 [5632, 2048], P('tp', 'fs'), may hold values from -0.078125 to 0.078125
- channel_post: float32 [2048], replicated, may hold values from 0.1 to 1.9
Outputs:
- layer_out: bfloat16 [16384, 2048], P('fs', 'tp')
The draws below stay inside these ranges and needn't reach their ends.
All inputs are finite; a program needn't handle non-finite values.
Results may differ from the reference program's by a relative error of at most 0.018.
Values may be sent and summed in bfloat16 or wider, within the bound.
No kernel may reach another device: no remote copies, remote signals or barrier semaphores. Data moves between devices by JAX's collectives and lax.ppermute only.
A program may use at most 64 MiB of HBM per device.

```python
import math
import jax
import jax.numpy as jnp
from jax import lax

D = 2048
RNN = 1024
BLOCK = 64
CONV = 4
FF = 5632
TOK_DEV = 512
BLOCKS = 16
TOKENS = 16384
PARTS_SIZE = 8
N_FS = 32


def draw_tokens(key, part):
    base_key = jax.random.fold_in(key, 11)
    span_key = jax.random.fold_in(key, 12)
    span_count = (TOKENS + 31) // 32
    base_draw = jnp.clip(jax.random.normal(base_key, (TOKENS, D), jnp.float32), -4.0, 4.0)
    offset = jnp.clip(jax.random.normal(span_key, (span_count, D), jnp.float32), -2.0, 2.0)
    shifted = base_draw + jnp.repeat(offset, 32, axis=0)[:TOKENS]
    return shifted.astype(jnp.bfloat16)


def draw_decay_param(key, part):
    pick_key = jax.random.fold_in(key, 21)
    slow_key = jax.random.fold_in(key, 22)
    fast_key = jax.random.fold_in(key, 23)
    slow_share = 0.5
    slow_mask = jax.random.uniform(pick_key, (2, RNN), jnp.float32) < slow_share
    slow_rate = jnp.exp(jax.random.uniform(slow_key, (2, RNN), jnp.float32, math.log(0.05 / TOK_DEV), math.log(0.3 / TOK_DEV)))
    fast_rate = jnp.exp(jax.random.uniform(fast_key, (2, RNN), jnp.float32, math.log(1.0 / 400.0), math.log(1.0 / 120.0)))
    chosen = jnp.where(slow_mask, slow_rate, fast_rate)
    return (-jnp.log(jnp.expm1(chosen))).astype(jnp.float32)


def level_of(stream_key, dims, pieces, smallest, high):
    def one(axis_at, blocks):
        steps = jax.random.uniform(jax.random.fold_in(jax.random.fold_in(stream_key, 6), axis_at), (blocks,), jnp.float32, smallest / len(pieces), high / len(pieces))
        return jnp.repeat(jnp.exp(steps), dims[axis_at] // blocks).reshape((-1,) + (1,) * (len(dims) - axis_at - 1))

    level = one(*pieces[0])
    for cut in pieces[1:]:
        level = level * one(*cut)
    return level


def noise(key, extent, deviation, most, cuts=(), dtype=jnp.bfloat16):
    drawn = deviation * jax.random.normal(key, extent, jnp.float32)
    if cuts:
        drawn = drawn * level_of(key, extent, cuts, -0.22, 0.18)
    return jnp.clip(drawn, -most, most).astype(dtype)


def setup_inputs(seed: int = 0) -> dict:
    arg_keys = jax.random.split(jax.random.key(seed), 17)
    tokens = draw_tokens(jax.random.fold_in(arg_keys[16], 71), 0)
    mixer_gain = jnp.clip(1.0 + 0.18 * jax.random.normal(arg_keys[1], (D,), jnp.float32), 0.1, 1.9)
    recur_in = noise(arg_keys[2], (D, RNN), D ** -0.5, 0.125, ((0, 32), (1, 8)))
    branch_in = noise(arg_keys[3], (D, RNN), D ** -0.5, 0.125, ((0, 32), (1, 8)))
    conv_taps = noise(arg_keys[4], (CONV, RNN), CONV ** -0.5, 3.0)
    recur_gate = noise(arg_keys[5], (2, BLOCKS, BLOCK, BLOCK), BLOCK ** -0.5, 0.75)
    input_gate = noise(arg_keys[6], (2, BLOCKS, BLOCK, BLOCK), BLOCK ** -0.5, 0.75)
    decay_param = draw_decay_param(jax.random.fold_in(arg_keys[16], 71), 0)
    recur_gain = jnp.clip(1.0 + 0.18 * jax.random.normal(arg_keys[8], (RNN,), jnp.float32), 0.1, 1.9)
    recur_out = noise(arg_keys[9], (RNN, D), RNN ** -0.5, 0.1875, ((0, 8), (1, 32)))
    mixer_post = jnp.clip(1.0 + 0.18 * jax.random.normal(arg_keys[10], (D,), jnp.float32), 0.1, 1.9)
    channel_gain = jnp.clip(1.0 + 0.18 * jax.random.normal(arg_keys[11], (D,), jnp.float32), 0.1, 1.9)
    hidden_gate = noise(arg_keys[12], (D, FF), D ** -0.5, 0.125, ((0, 32), (1, 8)))
    hidden_up = noise(arg_keys[13], (D, FF), D ** -0.5, 0.125, ((0, 32), (1, 8)))
    hidden_down = noise(arg_keys[14], (FF, D), FF ** -0.5, 0.078125, ((0, 8), (1, 32)))
    channel_post = jnp.clip(1.0 + 0.18 * jax.random.normal(arg_keys[15], (D,), jnp.float32), 0.1, 1.9)
    return {"tokens": tokens, "mixer_gain": mixer_gain, "recur_in": recur_in, "branch_in": branch_in, "conv_taps": conv_taps, "recur_gate": recur_gate, "input_gate": input_gate, "decay_param": decay_param, "recur_gain": recur_gain, "recur_out": recur_out, "mixer_post": mixer_post, "channel_gain": channel_gain, "hidden_gate": hidden_gate, "hidden_up": hidden_up, "hidden_down": hidden_down, "channel_post": channel_post}


EPS = 1e-06
SHRINK = 8.0

def rms_scale(values, gain):
    return values * lax.rsqrt(lax.optimization_barrier(jnp.mean(values * values, axis=-1, keepdims=True)) + EPS) * gain

def linear_scan(decay, inflow, reverse):

    def combine(former, latter):
        return (former[0] * latter[0], latter[0] * former[1] + latter[1])
    return lax.associative_scan(combine, (decay, inflow), axis=0, reverse=reverse)[1]

def short_conv(recur_x, taps):
    length = recur_x.shape[0]
    padded = jnp.pad(recur_x.astype(jnp.float32), ((2, 1), (0, 0)))
    total = taps[0] * padded[0:length]
    for position in range(1, taps.shape[0]):
        total = total + taps[position] * padded[position:position + length]
    return total

def recurrence(conv_out, rate_weight, inlet_weight, decay_row, reverse):
    length, width = conv_out.shape
    grouped = conv_out.reshape(length, rate_weight.shape[0], rate_weight.shape[1])
    rate = jax.nn.sigmoid(jnp.einsum('lhi,hij->lhj', grouped, rate_weight.astype(jnp.float32), precision=lax.Precision.HIGHEST).reshape(length, width))
    inlet = jax.nn.sigmoid(jnp.einsum('lhi,hij->lhj', grouped, inlet_weight.astype(jnp.float32), precision=lax.Precision.HIGHEST).reshape(length, width))
    log_decay = -SHRINK * rate * jax.nn.softplus(-decay_row)
    inflow = conv_out * inlet * jnp.sqrt(-jnp.expm1(2.0 * log_decay))
    return linear_scan(jnp.exp(log_decay), inflow, reverse)

def grouped_product(left, right, groups):
    length = left.shape[0]
    inner = left.shape[1] // groups
    left_groups = left.astype(jnp.float32).reshape(length, groups, inner)
    right_groups = right.astype(jnp.float32).reshape(groups, inner, right.shape[1])
    partial_value = jnp.einsum('lgk,gkd->gld', left_groups, right_groups, precision=lax.Precision.HIGHEST)
    rounded = lax.optimization_barrier(partial_value.astype(jnp.bfloat16))
    return lax.optimization_barrier(jnp.sum(rounded.astype(jnp.float32), axis=0))

def reference(tokens, mixer_gain, recur_in, branch_in, conv_taps, recur_gate, input_gate, decay_param, recur_gain, recur_out, mixer_post, channel_gain, hidden_gate, hidden_up, hidden_down, channel_post):
    taps = conv_taps.astype(jnp.float32)

    def one_sequence(sequence):
        seq_float = sequence.astype(jnp.float32)
        normed_in = rms_scale(seq_float, mixer_gain).astype(jnp.bfloat16)
        recur_x = jnp.dot(normed_in, recur_in, preferred_element_type=jnp.float32).astype(jnp.bfloat16)
        branch_x = jnp.dot(normed_in, branch_in, preferred_element_type=jnp.float32).astype(jnp.bfloat16)
        conv_out = short_conv(recur_x, taps)
        forward = recurrence(conv_out, recur_gate[0], input_gate[0], decay_param[0], False)
        backward = recurrence(conv_out, recur_gate[1], input_gate[1], decay_param[1], True)
        mixed = (forward + backward) * jax.nn.gelu(branch_x.astype(jnp.float32))
        recur_y = (mixed * recur_gain).astype(jnp.bfloat16)
        branch_sum = grouped_product(recur_y, recur_out, PARTS_SIZE)
        res_mid = (seq_float + rms_scale(branch_sum, mixer_post)).astype(jnp.bfloat16)
        mid_float = res_mid.astype(jnp.float32)
        channel_in = rms_scale(mid_float, channel_gain).astype(jnp.bfloat16)
        gate = jnp.dot(channel_in, hidden_gate, preferred_element_type=jnp.float32)
        up_value = jnp.dot(channel_in, hidden_up, preferred_element_type=jnp.float32)
        hidden = (jax.nn.silu(gate) * up_value).astype(jnp.bfloat16)
        hidden_sum = grouped_product(hidden, hidden_down, PARTS_SIZE)
        return (mid_float + rms_scale(hidden_sum, channel_post)).astype(jnp.bfloat16)
    result = lax.map(one_sequence, tokens.reshape(N_FS, TOK_DEV, D))
    return result.reshape(N_FS * TOK_DEV, D)
```

```python
import jax
import jax.numpy as jnp
from jax import lax
from jax.experimental import pallas as pl
from jax.experimental.pallas import tpu as pltpu
from jax.sharding import Mesh
from jax.sharding import PartitionSpec as P

D = 2048
BLOCK = 64
FS = ("z", "y")
TP = ("x", "c")
EPS = 1e-06
SHRINK = 8.0
SEG = 64
PAD_SEG = 72


def shift(array, axis, by):
    n = lax.axis_size(axis)
    return lax.ppermute(array, axis, [(i, (i + by) % n) for i in range(n)])


def swap_cores(array):
    return lax.ppermute(array, "c", [(0, 1), (1, 0)])


def from_all_x(array):
    return [array] + [shift(array, "x", k) for k in (1, 2, 3)]


def along_y(shard):
    y = lax.axis_index("y")
    n = lax.axis_size("y")
    rows = shard.shape[0]
    whole = jnp.zeros((n * rows, *shard.shape[1:]), shard.dtype)
    for k in range(n):
        piece = shard if k == 0 else shift(shard, "y", k)
        whole = lax.dynamic_update_slice_in_dim(whole, piece, ((y - k) % n) * rows, 0)
    return whole


def along_z(block):
    half = block.shape[0] // 2
    ahead, behind = [block], [block]
    for _ in range(3):
        ahead.append(shift(ahead[-1], "z", 1))
        behind.append(shift(behind[-1], "z", -1))
    low = shift(ahead[3][:half], "z", 1)
    high = shift(behind[3][half:], "z", -1)
    return ahead + [low, high] + behind[:0:-1]


def sigmoid(v):
    return 1.0 / (1.0 + jnp.exp(-v))


def one_minus_exp(v):
    series = jnp.ones_like(v)
    for n in range(9, 1, -1):
        series = 1.0 + v * (1.0 / n) * series
    return jnp.where(v > -0.5, -v * series, 1.0 - jnp.exp(v))


def nt_dot(left, right):
    return lax.dot_general(
        left, right, (((1,), (1,)), ((), ())), preferred_element_type=jnp.float32
    )


def recurrent_kernel(where, *refs):
    toks = refs[0:4]
    others = refs[4]
    gain, taps, gates, coef, out_gain = refs[5:10]
    blocks = refs[10:19]
    keep, send = refs[19:21]
    normed, w_in, w_out, padded, a_s, b_s, cum_s = refs[21:]
    x, c, z = where[0], where[1], where[2]
    chunks = [(toks[k], 2 * ((x - k) % 4) + c) for k in range(4)]
    chunks += [(others.at[k], 2 * ((x - k) % 4) + 1 - c) for k in range(4)]
    energy = None
    for ref, _ in chunks:
        v = ref[...].astype(jnp.float32)
        e = jnp.sum(v * v, axis=1, keepdims=True)
        energy = e if energy is None else energy + e
    scale = lax.rsqrt(energy / D + EPS)
    for ref, at in chunks:
        cols = pl.ds(pl.multiple_of(at * 256, 256), 256)
        v = ref[...].astype(jnp.float32)
        normed[:, cols] = (v * scale * gain[:, cols]).astype(jnp.bfloat16)
    row = 0
    for n, ref in enumerate(blocks):
        rows = ref.shape[0]
        k = (0, 1, 2, 3, 4, 4, 5, 6, 7)[n]
        start = ((z - k) % 8) * 256 + (128 if n == 5 else 0)
        at = pl.ds(pl.multiple_of(start, 128), rows)
        w_in[at, :] = ref[:, 0:256]
        w_out[at, :] = ref[:, 256:384]
    both = jnp.dot(normed[...], w_in[...], preferred_element_type=jnp.float32)
    recur_x = both[:, 0:128].astype(jnp.bfloat16).astype(jnp.float32)
    branch_x = both[:, 128:256].astype(jnp.bfloat16).astype(jnp.float32)
    length = recur_x.shape[0]
    padded[0:8, :] = jnp.zeros((8, 128), jnp.float32)
    padded[length + 8 : length + 16, :] = jnp.zeros((8, 128), jnp.float32)
    padded[8 : length + 8, :] = recur_x
    conv = taps[0:1, :] * padded[6 : length + 6, :]
    for k in range(1, 4):
        conv = conv + taps[k : k + 1, :] * padded[6 + k : length + 6 + k, :]
    weight = gates[...]
    high = conv.astype(jnp.bfloat16)
    rest = conv - high.astype(jnp.float32)
    mid = rest.astype(jnp.bfloat16)
    low = (rest - mid.astype(jnp.float32)).astype(jnp.bfloat16)
    mapped = (
        jnp.dot(low, weight, preferred_element_type=jnp.float32)
        + jnp.dot(mid, weight, preferred_element_type=jnp.float32)
    ) + jnp.dot(high, weight, preferred_element_type=jnp.float32)
    count = length // SEG
    for d in range(2):
        rate = sigmoid(mapped[:, d * 256 : d * 256 + 128])
        inlet = sigmoid(mapped[:, d * 256 + 128 : d * 256 + 256])
        log_decay = rate * coef[d : d + 1, :]
        inflow = conv * inlet * jnp.sqrt(one_minus_exp(2.0 * log_decay))
        decay = jnp.exp(log_decay)
        for s in range(count):
            a_s[d, s * PAD_SEG : s * PAD_SEG + SEG, :] = decay[s * SEG : s * SEG + SEG]
            b_s[d, s * PAD_SEG : s * PAD_SEG + SEG, :] = inflow[s * SEG : s * SEG + SEG]
    state = [jnp.zeros((count, 128), jnp.float32) for _ in range(2)]
    through = [jnp.ones((count, 128), jnp.float32) for _ in range(2)]
    for j in range(SEG):
        for d in range(2):
            at = pl.ds(j if d == 0 else SEG - 1 - j, count, stride=PAD_SEG)
            a = a_s[d, at, :]
            state[d] = a * state[d] + b_s[d, at, :]
            through[d] = a * through[d]
            b_s[d, at, :] = state[d]
            cum_s[d, at, :] = through[d]
    carries = [[None] * count for _ in range(2)]
    for d in range(2):
        order = list(range(count)) if d == 0 else list(range(count - 1, -1, -1))
        carry = jnp.zeros((1, 128), jnp.float32)
        for s in order:
            carries[d][s] = carry
            carry = through[d][s : s + 1] * carry + state[d][s : s + 1]
    summed = []
    for s in range(count):
        at = slice(s * PAD_SEG, s * PAD_SEG + SEG)
        summed.append(
            (b_s[0, at, :] + cum_s[0, at, :] * carries[0][s])
            + (b_s[1, at, :] + cum_s[1, at, :] * carries[1][s])
        )
    mixed = jnp.concatenate(summed, axis=0) * jax.nn.gelu(branch_x, approximate=True)
    recur_y = (mixed * out_gain[...]).astype(jnp.bfloat16)
    for to in range(4):
        mine = pl.ds(pl.multiple_of((2 * to + c) * 256, 256), 256)
        keep[to] = nt_dot(recur_y, w_out[mine, :]).astype(jnp.bfloat16)
        theirs = pl.ds(pl.multiple_of((2 * to + 1 - c) * 256, 256), 256)
        send[to] = nt_dot(recur_y, w_out[theirs, :]).astype(jnp.bfloat16)


def forward_kernel(where, *refs):
    toks = refs[0:4]
    tok_others = refs[4]
    sums = refs[5:9]
    sum_others = refs[9]
    post, gain = refs[10:12]
    w_in, w_out = refs[12:14]
    keep, send, mid_own = refs[14:17]
    mid, normed = refs[17:]
    x, c = where[0], where[1]
    chunks = [(toks[k], sums[k], 2 * ((x - k) % 4) + c) for k in range(4)]
    chunks += [
        (tok_others.at[k], sum_others.at[k], 2 * ((x - k) % 4) + 1 - c) for k in range(4)
    ]
    energy = None
    for _, ref, _ in chunks:
        v = ref[...].astype(jnp.float32)
        e = jnp.sum(v * v, axis=1, keepdims=True)
        energy = e if energy is None else energy + e
    scale = lax.rsqrt(energy / D + EPS)
    energy = None
    for tok, ref, at in chunks:
        cols = pl.ds(pl.multiple_of(at * 256, 256), 256)
        v = tok[...].astype(jnp.float32) + ref[...].astype(jnp.float32) * scale * post[:, cols]
        v = v.astype(jnp.bfloat16)
        mid[:, cols] = v
        if tok is toks[0]:
            mid_own[...] = v
        v = v.astype(jnp.float32)
        e = jnp.sum(v * v, axis=1, keepdims=True)
        energy = e if energy is None else energy + e
    scale = lax.rsqrt(energy / D + EPS)
    for at in range(8):
        cols = slice(at * 256, at * 256 + 256)
        normed[:, cols] = (mid[:, cols].astype(jnp.float32) * scale * gain[:, cols]).astype(
            jnp.bfloat16
        )
    both = jnp.dot(normed[...], w_in[...], preferred_element_type=jnp.float32)
    width = both.shape[1] // 2
    gate = both[:, :width]
    hidden = (gate * sigmoid(gate) * both[:, width:]).astype(jnp.bfloat16)
    for to in range(4):
        mine = pl.ds(pl.multiple_of((2 * to + c) * 256, 256), 256)
        keep[to] = nt_dot(hidden, w_out[mine, :]).astype(jnp.bfloat16)
        theirs = pl.ds(pl.multiple_of((2 * to + 1 - c) * 256, 256), 256)
        send[to] = nt_dot(hidden, w_out[theirs, :]).astype(jnp.bfloat16)


VMEM = pl.BlockSpec(memory_space=pltpu.MemorySpace.VMEM)
SMEM = pl.BlockSpec(memory_space=pltpu.MemorySpace.SMEM)


def pieces(length):
    return jax.ShapeDtypeStruct((4, length, 256), jnp.bfloat16)


def sum_at_owner(keep, send):
    x = lax.axis_index("x")
    came = swap_cores(send)

    def pair(to):
        one = lax.dynamic_index_in_dim(keep, to, 0, False).astype(jnp.float32)
        two = lax.dynamic_index_in_dim(came, to, 0, False).astype(jnp.float32)
        return one + two

    total = pair(x)
    for k in (1, 2, 3):
        total = total + shift(pair((x + k) % 4).astype(jnp.bfloat16), "x", k).astype(jnp.float32)
    return total


def on_device(
    tokens,
    mixer_gain,
    recur_in,
    branch_in,
    conv_taps,
    recur_gate,
    input_gate,
    decay_param,
    recur_gain,
    recur_out,
    mixer_post,
    channel_gain,
    hidden_gate,
    hidden_up,
    hidden_down,
    channel_post,
):
    x, c, z = lax.axis_index("x"), lax.axis_index("c"), lax.axis_index("z")
    rank_tp = 2 * x + c
    length, feature_width = tokens.shape
    channels = recur_in.shape[1]
    groups = channels // BLOCK
    where = jnp.stack([x, c, z]).astype(jnp.int32)

    hidden_shard = jnp.concatenate([hidden_gate, hidden_up, hidden_down.T], axis=1)
    hidden_all = lax.all_gather(hidden_shard, FS, axis=0, tiled=True)

    recur_shard = jnp.concatenate([recur_in, branch_in, recur_out.T], axis=1)
    blocks = along_z(along_y(recur_shard))
    toks = from_all_x(tokens)
    tok_others = swap_cores(jnp.stack(toks))

    taps = lax.dynamic_slice_in_dim(conv_taps, rank_tp * channels, channels, 1).astype(jnp.float32)
    rate = lax.dynamic_slice_in_dim(recur_gate, rank_tp * groups, groups, 1)
    inlet = lax.dynamic_slice_in_dim(input_gate, rank_tp * groups, groups, 1)
    empty = jnp.zeros((BLOCK, BLOCK), jnp.bfloat16)
    upper, lower = [], []
    for d in range(2):
        for kind in (rate, inlet):
            upper += [kind[d, 0], empty]
            lower += [empty, kind[d, 1]]
    gates = jnp.concatenate(
        [jnp.concatenate(upper, axis=1), jnp.concatenate(lower, axis=1)], axis=0
    )
    decay_own = lax.dynamic_slice_in_dim(decay_param, rank_tp * channels, channels, 1)
    coef = -SHRINK * jax.nn.softplus(-decay_own)
    gain_own = lax.dynamic_slice_in_dim(recur_gain, rank_tp * channels, channels, 0)

    seg_rows = (length // SEG) * PAD_SEG
    keep, send = pl.pallas_call(
        recurrent_kernel,
        out_shape=(pieces(length), pieces(length)),
        in_specs=[SMEM] + [VMEM] * 19,
        out_specs=(VMEM, VMEM),
        scratch_shapes=[
            pltpu.VMEM((length, D), jnp.bfloat16),
            pltpu.VMEM((D, 256), jnp.bfloat16),
            pltpu.VMEM((D, 128), jnp.bfloat16),
            pltpu.VMEM((length + 16, channels), jnp.float32),
            pltpu.VMEM((2, seg_rows, channels), jnp.float32),
            pltpu.VMEM((2, seg_rows, channels), jnp.float32),
            pltpu.VMEM((2, seg_rows, channels), jnp.float32),
        ],
        name="recurrent",
    )(
        where,
        *toks,
        tok_others,
        mixer_gain[None],
        taps,
        gates,
        coef,
        gain_own[None],
        *blocks,
    )
    branch_own = sum_at_owner(keep, send).astype(jnp.bfloat16)
    sums = from_all_x(branch_own)
    sum_others = swap_cores(jnp.stack(sums))
    width = 2 * hidden_gate.shape[1]
    keep, send, mid_own = pl.pallas_call(
        forward_kernel,
        out_shape=(
            pieces(length),
            pieces(length),
            jax.ShapeDtypeStruct((length, feature_width), jnp.bfloat16),
        ),
        in_specs=[SMEM] + [VMEM] * 14,
        out_specs=(VMEM, VMEM, VMEM),
        scratch_shapes=[
            pltpu.VMEM((length, D), jnp.bfloat16),
            pltpu.VMEM((length, D), jnp.bfloat16),
        ],
        name="forward",
    )(
        where,
        *toks,
        tok_others,
        *sums,
        sum_others,
        mixer_post[None],
        channel_gain[None],
        hidden_all[:, :width],
        hidden_all[:, width:],
    )
    hidden_own = sum_at_owner(keep, send)
    energy = jnp.sum(hidden_own * hidden_own, axis=1)
    everyone = jnp.broadcast_to(energy, (8, length))
    energy = jnp.sum(lax.all_to_all(everyone, TP, 0, 0, tiled=True), axis=0)
    post_own = lax.dynamic_slice_in_dim(channel_post, rank_tp * feature_width, feature_width, 0)
    return (
        mid_own.astype(jnp.float32)
        + hidden_own * lax.rsqrt(energy / D + EPS)[:, None] * post_own
    ).astype(jnp.bfloat16)


def solution(mesh):
    split = Mesh(mesh.devices.reshape(8, 4, 4, 2), ("z", "y", "x", "c"))
    placed = (
        P(FS, TP),
        P(),
        P(FS, TP),
        P(FS, TP),
        P(),
        P(),
        P(),
        P(),
        P(),
        P(TP, FS),
        P(),
        P(),
        P(FS, TP),
        P(FS, TP),
        P(TP, FS),
        P(),
    )
    return jax.shard_map(
        on_device, mesh=split, in_specs=placed, out_specs=P(FS, TP), check_vma=False
    )
```

```python
import jax
import jax.numpy as jnp
from jax import lax
from jax.experimental import pallas as pl
from jax.experimental.pallas import tpu as pltpu
from jax.sharding import Mesh
from jax.sharding import PartitionSpec as P

D = 2048
BLOCK = 64
FS = ("z", "y")
TP = ("x", "c")
EPS = 1e-06
SHRINK = 8.0
SEG = 64
PAD_SEG = 72


def shift(array, axis, by):
    n = lax.axis_size(axis)
    return lax.ppermute(array, axis, [(i, (i + by) % n) for i in range(n)])


def swap_cores(array):
    return lax.ppermute(array, "c", [(0, 1), (1, 0)])


def from_all_x(array):
    return [array] + [shift(array, "x", k) for k in (1, 2, 3)]


def from_all_y(array):
    return [array] + [shift(array, "y", k) for k in (1, 2, 3)]


def along_z(block):
    half = block.shape[0] // 2
    ahead, behind = [block], [block]
    for _ in range(3):
        ahead.append(shift(ahead[-1], "z", 1))
        behind.append(shift(behind[-1], "z", -1))
    low = shift(ahead[3][:half], "z", 1)
    high = shift(behind[3][half:], "z", -1)
    return ahead + [low, high] + behind[:0:-1]


def own_rows(z, y, back_z, back_y):
    return pl.multiple_of((((z - back_z) % 8) * 4 + (y - back_y) % 4) * 64, 64)


def pack_kernel(recur_in, branch_in, recur_out_t, gate, up, down_t, narrow, wide):
    wide[:, 0:704] = gate[...]
    wide[:, 704:1408] = up[...]
    narrow[0:64] = recur_out_t[...]
    narrow[64:128] = recur_in[...]
    narrow[128:192] = branch_in[...]
    for t in range(5):
        narrow[192 + t * 64 : 256 + t * 64] = down_t[:, t * 128 : t * 128 + 128]
    narrow[512:544, 0:64] = down_t[0:32, 640:704]
    narrow[512:544, 64:128] = down_t[32:64, 640:704]


def split_kernel(*refs):
    out, inner, down = refs[9:]
    for n, ref in enumerate(refs[:9]):
        k = (0, 1, 2, 3, 4, 4, 5, 6, 7)[n]
        if n == 4:
            out[256:320, :] = ref[0:64, :]
            inner[512:640, :] = ref[64:192, :]
            down[1408:1488, :] = ref[192:272, :]
        elif n == 5:
            down[1488:1760, :] = ref[...]
        else:
            out[k * 64 : k * 64 + 64, :] = ref[0:64, :]
            inner[k * 128 : k * 128 + 128, :] = ref[64:192, :]
            down[k * 352 : k * 352 + 352, :] = ref[192:544, :]


def stack_kernel(*refs):
    rows = refs[0].shape[0]
    for k in range(4):
        refs[4][k * rows : k * rows + rows, :] = refs[k][...]


def join_kernel(where, *refs):
    y = where[3]
    for k in range(4):
        refs[4][pl.ds(pl.multiple_of(((y - k) % 4) * 64, 64), 64), :] = refs[k][...]


def sigmoid(v):
    return 1.0 / (1.0 + jnp.exp(-v))


def one_minus_exp(v):
    series = jnp.ones_like(v)
    for n in range(9, 1, -1):
        series = 1.0 + v * (1.0 / n) * series
    return jnp.where(v > -0.5, -v * series, 1.0 - jnp.exp(v))


def nt_dot(left, right):
    return lax.dot_general(
        left, right, (((1,), (1,)), ((), ())), preferred_element_type=jnp.float32
    )


def recurrent_kernel(where, *refs):
    toks = refs[0:4]
    others = refs[4]
    gain, conv_taps, recur_gate, input_gate, coefs, out_gains = refs[5:11]
    pieces_in = refs[11:15]
    recur_out = refs[15]
    normed, w_in, gates, padded, a_s, b_s, cum_s = refs[16:]
    x, c, z, y = where[0], where[1], where[2], where[3]
    own = pl.ds(pl.multiple_of((2 * x + c) * 128, 128), 128)
    taps = conv_taps[:, own].astype(jnp.float32)
    coef = coefs[:, own]
    out_gain = out_gains[:, own]
    gates[...] = jnp.zeros(gates.shape, jnp.bfloat16)
    for d in range(2):
        for kind, ref in enumerate((recur_gate, input_gate)):
            for g in range(2):
                first = (2 * d + kind) * 128 + g * BLOCK
                gates[g * BLOCK : (g + 1) * BLOCK, first : first + BLOCK] = ref[
                    d, 2 * (2 * x + c) + g
                ]
    chunks = [(toks[k], 2 * ((x - k) % 4) + c) for k in range(4)]
    chunks += [(others.at[k], 2 * ((x - k) % 4) + 1 - c) for k in range(4)]
    energy = None
    for ref, _ in chunks:
        v = ref[...].astype(jnp.float32)
        e = jnp.sum(v * v, axis=1, keepdims=True)
        energy = e if energy is None else energy + e
    scale = lax.rsqrt(energy / D + EPS)
    for ref, at in chunks:
        cols = pl.ds(pl.multiple_of(at * 256, 256), 256)
        v = ref[...].astype(jnp.float32)
        normed[:, cols] = (v * scale * gain[:, cols]).astype(jnp.bfloat16)
    for back_y, ref in enumerate(pieces_in):
        for back_z in range(8):
            at = pl.ds(own_rows(z, y, back_z, back_y), 64)
            w_in[at, 0:128] = ref[back_z * 128 : back_z * 128 + 64, :]
            w_in[at, 128:256] = ref[back_z * 128 + 64 : back_z * 128 + 128, :]
    both = jnp.dot(normed[...], w_in[...], preferred_element_type=jnp.float32)
    recur_x = both[:, 0:128].astype(jnp.bfloat16).astype(jnp.float32)
    branch_x = both[:, 128:256].astype(jnp.bfloat16).astype(jnp.float32)
    length = recur_x.shape[0]
    padded[0:8, :] = jnp.zeros((8, 128), jnp.float32)
    padded[length + 8 : length + 16, :] = jnp.zeros((8, 128), jnp.float32)
    padded[8 : length + 8, :] = recur_x
    conv = taps[0:1, :] * padded[6 : length + 6, :]
    for k in range(1, 4):
        conv = conv + taps[k : k + 1, :] * padded[6 + k : length + 6 + k, :]
    weight = gates[...]
    high = conv.astype(jnp.bfloat16)
    rest = conv - high.astype(jnp.float32)
    mid = rest.astype(jnp.bfloat16)
    low = (rest - mid.astype(jnp.float32)).astype(jnp.bfloat16)
    mapped = (
        jnp.dot(low, weight, preferred_element_type=jnp.float32)
        + jnp.dot(mid, weight, preferred_element_type=jnp.float32)
    ) + jnp.dot(high, weight, preferred_element_type=jnp.float32)
    count = length // SEG
    for d in range(2):
        rate = sigmoid(mapped[:, d * 256 : d * 256 + 128])
        inlet = sigmoid(mapped[:, d * 256 + 128 : d * 256 + 256])
        log_decay = rate * coef[d : d + 1, :]
        inflow = conv * inlet * jnp.sqrt(one_minus_exp(2.0 * log_decay))
        decay = jnp.exp(log_decay)
        for s in range(count):
            a_s[d, s * PAD_SEG : s * PAD_SEG + SEG, :] = decay[s * SEG : s * SEG + SEG]
            b_s[d, s * PAD_SEG : s * PAD_SEG + SEG, :] = inflow[s * SEG : s * SEG + SEG]
    state = [jnp.zeros((count, 128), jnp.float32) for _ in range(2)]
    through = [jnp.ones((count, 128), jnp.float32) for _ in range(2)]
    for j in range(SEG):
        for d in range(2):
            at = pl.ds(j if d == 0 else SEG - 1 - j, count, stride=PAD_SEG)
            a = a_s[d, at, :]
            state[d] = a * state[d] + b_s[d, at, :]
            through[d] = a * through[d]
            b_s[d, at, :] = state[d]
            cum_s[d, at, :] = through[d]
    carries = [[None] * count for _ in range(2)]
    for d in range(2):
        order = list(range(count)) if d == 0 else list(range(count - 1, -1, -1))
        carry = jnp.zeros((1, 128), jnp.float32)
        for s in order:
            carries[d][s] = carry
            carry = through[d][s : s + 1] * carry + state[d][s : s + 1]
    summed = []
    for s in range(count):
        at = slice(s * PAD_SEG, s * PAD_SEG + SEG)
        summed.append(
            (b_s[0, at, :] + cum_s[0, at, :] * carries[0][s])
            + (b_s[1, at, :] + cum_s[1, at, :] * carries[1][s])
        )
    mixed = jnp.concatenate(summed, axis=0) * jax.nn.gelu(branch_x, approximate=True)
    recur_out[...] = (mixed * out_gain).astype(jnp.bfloat16)


def middle_kernel(where, *refs):
    toks = refs[0:4]
    tok_others = refs[4]
    recur = refs[5:9]
    recur_others = refs[9]
    weights = refs[10:14]
    weight_others = refs[14]
    post, gain = refs[15:17]
    normed, mid_own = refs[17:19]
    left, right, mid = refs[19:]
    x, c, z, y = where[0], where[1], where[2], where[3]
    for k in range(4):
        left[:, k * 128 : k * 128 + 128] = recur[k][...]
        left[:, 512 + k * 128 : 640 + k * 128] = recur_others[k]
        for back_y in range(4):
            for back_z in range(8):
                at = pl.ds(own_rows(z, y, back_z, back_y), 64)
                come = slice((back_y * 8 + back_z) * 64, (back_y * 8 + back_z) * 64 + 64)
                right[at, k * 128 : k * 128 + 128] = weights[k][come, :]
                right[at, 512 + k * 128 : 640 + k * 128] = weight_others[k, come, :]
    total = nt_dot(left[...], right[...])
    scale = lax.rsqrt(jnp.sum(total * total, axis=1, keepdims=True) / D + EPS)
    mid[...] = total * scale * post[...]
    chunks = [(toks[k], 2 * ((x - k) % 4) + c) for k in range(4)]
    chunks += [(tok_others.at[k], 2 * ((x - k) % 4) + 1 - c) for k in range(4)]
    energy = None
    for tok, at in chunks:
        cols = pl.ds(pl.multiple_of(at * 256, 256), 256)
        v = (tok[...].astype(jnp.float32) + mid[:, cols]).astype(jnp.bfloat16)
        if tok is toks[0]:
            mid_own[...] = v
        v = v.astype(jnp.float32)
        mid[:, cols] = v
        e = jnp.sum(v * v, axis=1, keepdims=True)
        energy = e if energy is None else energy + e
    scale = lax.rsqrt(energy / D + EPS)
    for at in range(8):
        cols = slice(at * 256, at * 256 + 256)
        normed[:, cols] = (mid[:, cols] * scale * gain[:, cols]).astype(jnp.bfloat16)


def forward_kernel(where, *refs):
    normed = refs[0]
    blocks = refs[1:10]
    pieces_in = refs[10:14]
    send, hidden, w_out = refs[14:17]
    w_in = refs[17]
    c, z, y = where[1], where[2], where[3]
    for n, ref in enumerate(blocks):
        k = (0, 1, 2, 3, 4, 4, 5, 6, 7)[n]
        start = ((z - k) % 8) * 256 + (128 if n == 5 else 0)
        w_in[pl.ds(pl.multiple_of(start, 128), ref.shape[0]), :] = ref[...]
    for back_z in range(8):
        at_z = (z - back_z) % 8
        core, at_x = at_z % 2, at_z // 2
        for back_y, ref in enumerate(pieces_in):
            first = pl.multiple_of(at_x * 256 + ((y - back_y) % 4) * 64, 64)
            come = back_z * 352
            for t in range(5):
                w_out[core, pl.ds(first, 64), t * 128 : t * 128 + 128] = ref[
                    come + t * 64 : come + t * 64 + 64, :
                ]
            last = ref[come + 320 : come + 352, :]
            w_out[core, pl.ds(first, 32), 640:704] = last[:, 0:64]
            w_out[core, pl.ds(first + 32, 32), 640:704] = last[:, 64:128]
    both = jnp.dot(normed[...], w_in[...], preferred_element_type=jnp.float32)
    width = both.shape[1] // 2
    gate = both[:, :width]
    hidden[...] = (gate * sigmoid(gate) * both[:, width:]).astype(jnp.bfloat16)
    for to in range(4):
        rows = slice(to * 256, to * 256 + 256)
        send[to] = nt_dot(hidden[...], w_out[1 - c, rows, :]).astype(jnp.bfloat16)


def last_kernel(where, hidden, w_out, came, own, one, two, three):
    x, c = where[0], where[1]
    for k, ref in enumerate((own, one, two, three)):
        to = (x + k) % 4
        rows = pl.ds(pl.multiple_of(to * 256, 256), 256)
        pair = nt_dot(hidden[...], w_out[c, rows, :]) + came[to].astype(jnp.float32)
        ref[...] = pair.astype(ref.dtype)


VMEM = pl.BlockSpec(memory_space=pltpu.MemorySpace.VMEM)
SMEM = pl.BlockSpec(memory_space=pltpu.MemorySpace.SMEM)


def on_device(
    tokens,
    mixer_gain,
    recur_in,
    branch_in,
    conv_taps,
    recur_gate,
    input_gate,
    decay_param,
    recur_gain,
    recur_out,
    mixer_post,
    channel_gain,
    hidden_gate,
    hidden_up,
    hidden_down,
    channel_post,
):
    x, c = lax.axis_index("x"), lax.axis_index("c")
    rank_tp = 2 * x + c
    length, feature_width = tokens.shape
    channels = recur_in.shape[1]
    rows = recur_in.shape[0]
    width = hidden_gate.shape[1]
    where = jnp.stack([x, c, lax.axis_index("z"), lax.axis_index("y")]).astype(jnp.int32)

    narrow, wide = pl.pallas_call(
        pack_kernel,
        out_shape=(
            jax.ShapeDtypeStruct((3 * rows + width // 2, 128), jnp.bfloat16),
            jax.ShapeDtypeStruct((rows, 2 * width), jnp.bfloat16),
        ),
        in_specs=[VMEM] * 6,
        out_specs=(VMEM, VMEM),
        name="pack",
    )(recur_in, branch_in, recur_out.T, hidden_gate, hidden_up, hidden_down.T)
    out_z, in_z, down_z = pl.pallas_call(
        split_kernel,
        out_shape=(
            jax.ShapeDtypeStruct((8 * rows, 128), jnp.bfloat16),
            jax.ShapeDtypeStruct((16 * rows, 128), jnp.bfloat16),
            jax.ShapeDtypeStruct((4 * width, 128), jnp.bfloat16),
        ),
        in_specs=[VMEM] * 9,
        out_specs=(VMEM,) * 3,
        name="split",
    )(*along_z(narrow))
    wide_y = from_all_y(wide)
    hidden_y = pl.pallas_call(
        join_kernel,
        out_shape=jax.ShapeDtypeStruct((4 * rows, 2 * width), jnp.bfloat16),
        in_specs=[SMEM] + [VMEM] * 4,
        out_specs=VMEM,
        name="join",
    )(where, *wide_y)
    toks = from_all_x(tokens)
    hidden_blocks = along_z(hidden_y)
    tok_others = swap_cores(jnp.stack(toks))
    out_y = from_all_y(out_z)
    in_y = from_all_y(in_z)
    down_y = from_all_y(down_z)
    weights = pl.pallas_call(
        stack_kernel,
        out_shape=jax.ShapeDtypeStruct((D, 128), jnp.bfloat16),
        in_specs=[VMEM] * 4,
        out_specs=VMEM,
        name="stack",
    )(*out_y)
    weights = from_all_x(weights)
    weight_others = swap_cores(jnp.stack(weights))
    coef = -SHRINK * jax.nn.softplus(-decay_param)

    seg_rows = (length // SEG) * PAD_SEG
    recur_y = pl.pallas_call(
        recurrent_kernel,
        out_shape=jax.ShapeDtypeStruct((length, channels), jnp.bfloat16),
        in_specs=[SMEM] + [VMEM] * 15,
        out_specs=VMEM,
        scratch_shapes=[
            pltpu.VMEM((length, D), jnp.bfloat16),
            pltpu.VMEM((D, 256), jnp.bfloat16),
            pltpu.VMEM((channels, 4 * channels), jnp.bfloat16),
            pltpu.VMEM((length + 16, channels), jnp.float32),
            pltpu.VMEM((2, seg_rows, channels), jnp.float32),
            pltpu.VMEM((2, seg_rows, channels), jnp.float32),
            pltpu.VMEM((2, seg_rows, channels), jnp.float32),
        ],
        name="recurrent",
    )(
        where,
        *toks,
        tok_others,
        mixer_gain[None],
        conv_taps,
        recur_gate,
        input_gate,
        coef,
        recur_gain[None],
        *in_y,
    )
    recur = from_all_x(recur_y)
    recur_others = swap_cores(jnp.stack(recur))
    normed, mid_own = pl.pallas_call(
        middle_kernel,
        out_shape=(
            jax.ShapeDtypeStruct((length, D), jnp.bfloat16),
            jax.ShapeDtypeStruct((length, feature_width), jnp.bfloat16),
        ),
        in_specs=[SMEM] + [VMEM] * 17,
        out_specs=(VMEM, VMEM),
        scratch_shapes=[
            pltpu.VMEM((length, 8 * channels), jnp.bfloat16),
            pltpu.VMEM((D, 8 * channels), jnp.bfloat16),
            pltpu.VMEM((length, D), jnp.float32),
        ],
        name="middle",
    )(
        where,
        *toks,
        tok_others,
        *recur,
        recur_others,
        *weights,
        weight_others,
        mixer_post[None],
        channel_gain[None],
    )
    send, hidden, w_out = pl.pallas_call(
        forward_kernel,
        out_shape=(
            jax.ShapeDtypeStruct((4, length, 256), jnp.bfloat16),
            jax.ShapeDtypeStruct((length, width), jnp.bfloat16),
            jax.ShapeDtypeStruct((2, D // 2, width), jnp.bfloat16),
        ),
        in_specs=[SMEM] + [VMEM] * 14,
        out_specs=(VMEM,) * 3,
        scratch_shapes=[pltpu.VMEM((D, 2 * width), jnp.bfloat16)],
        name="forward",
    )(where, normed, *hidden_blocks, *down_y)
    came = swap_cores(send)
    piece = (length, feature_width)
    hidden_own, one, two, three = pl.pallas_call(
        last_kernel,
        out_shape=(jax.ShapeDtypeStruct(piece, jnp.float32),)
        + (jax.ShapeDtypeStruct(piece, jnp.bfloat16),) * 3,
        in_specs=[SMEM] + [VMEM] * 3,
        out_specs=(VMEM,) * 4,
        name="last",
    )(where, hidden, w_out, came)
    for k, part in ((1, one), (2, two), (3, three)):
        hidden_own = hidden_own + shift(part, "x", k).astype(jnp.float32)
    energy = jnp.sum(hidden_own * hidden_own, axis=1)
    everyone = jnp.broadcast_to(energy, (8, length))
    energy = jnp.sum(lax.all_to_all(everyone, TP, 0, 0, tiled=True), axis=0)
    post_own = lax.dynamic_slice_in_dim(channel_post, rank_tp * feature_width, feature_width, 0)
    return (
        mid_own.astype(jnp.float32)
        + hidden_own * lax.rsqrt(energy / D + EPS)[:, None] * post_own
    ).astype(jnp.bfloat16)


def solution(mesh):
    split = Mesh(mesh.devices.reshape(8, 4, 4, 2), ("z", "y", "x", "c"))
    placed = (
        P(FS, TP),
        P(),
        P(FS, TP),
        P(FS, TP),
        P(),
        P(),
        P(),
        P(),
        P(),
        P(TP, FS),
        P(),
        P(),
        P(FS, TP),
        P(FS, TP),
        P(TP, FS),
        P(),
    )

    return jax.shard_map(on_device, mesh=split, in_specs=placed, out_specs=P(FS, TP), check_vma=False)
```

```python
import jax
import jax.numpy as jnp
from jax import lax
from jax.experimental import pallas as pl
from jax.experimental.pallas import tpu as pltpu
from jax.sharding import Mesh
from jax.sharding import PartitionSpec as P

D = 2048
BLOCK = 64
FS = ("z", "y")
TP = ("x", "c")
EPS = 1e-06
SHRINK = 8.0
SEG = 64
PAD_SEG = 72


def shift(array, axis, by):
    n = lax.axis_size(axis)
    return lax.ppermute(array, axis, [(i, (i + by) % n) for i in range(n)])


def swap_cores(array):
    return lax.ppermute(array, "c", [(0, 1), (1, 0)])


def from_all_x(array):
    return [array] + [shift(array, "x", k) for k in (1, 2, 3)]


def from_all_y(array):
    return [array] + [shift(array, "y", k) for k in (1, 2, 3)]


def along_z(block):
    half = block.shape[0] // 2
    ahead, behind = [block], [block]
    for _ in range(3):
        ahead.append(shift(ahead[-1], "z", 1))
        behind.append(shift(behind[-1], "z", -1))
    low = shift(ahead[3][:half], "z", 1)
    high = shift(behind[3][half:], "z", -1)
    return ahead + [low, high] + behind[:0:-1]


def own_rows(z, y, back_z, back_y):
    return pl.multiple_of((((z - back_z) % 8) * 4 + (y - back_y) % 4) * 64, 64)


def pack_kernel(recur_in, branch_in, recur_out_t, gate, up, down_t, narrow, wide):
    for t in range(5):
        wide[:, t * 256 : t * 256 + 128] = gate[:, t * 128 : t * 128 + 128]
        wide[:, t * 256 + 128 : t * 256 + 256] = up[:, t * 128 : t * 128 + 128]
    wide[:, 1280:1344] = gate[:, 640:704]
    wide[:, 1344:1408] = up[:, 640:704]
    narrow[0:64] = recur_out_t[...]
    narrow[64:128] = recur_in[...]
    narrow[128:192] = branch_in[...]
    for t in range(5):
        narrow[192 + t * 64 : 256 + t * 64] = down_t[:, t * 128 : t * 128 + 128]
    narrow[512:544, 0:64] = down_t[0:32, 640:704]
    narrow[512:544, 64:128] = down_t[32:64, 640:704]


def split_kernel(*refs):
    out, inner, down = refs[9:]
    for n, ref in enumerate(refs[:9]):
        k = (0, 1, 2, 3, 4, 4, 5, 6, 7)[n]
        if n == 4:
            out[256:320, :] = ref[0:64, :]
            inner[512:640, :] = ref[64:192, :]
            down[1408:1488, :] = ref[192:272, :]
        elif n == 5:
            down[1488:1760, :] = ref[...]
        else:
            out[k * 64 : k * 64 + 64, :] = ref[0:64, :]
            inner[k * 128 : k * 128 + 128, :] = ref[64:192, :]
            down[k * 352 : k * 352 + 352, :] = ref[192:544, :]


def stack_kernel(*refs):
    rows = refs[0].shape[0]
    for k in range(4):
        refs[4][k * rows : k * rows + rows, :] = refs[k][...]


def join_kernel(where, *refs):
    y = where[3]
    for k in range(4):
        refs[4][pl.ds(pl.multiple_of(((y - k) % 4) * 64, 64), 64), :] = refs[k][...]


def sigmoid(v):
    return 1.0 / (1.0 + jnp.exp(-v))


def one_minus_exp(v):
    series = jnp.ones_like(v)
    for n in range(9, 1, -1):
        series = 1.0 + v * (1.0 / n) * series
    return jnp.where(v > -0.5, -v * series, 1.0 - jnp.exp(v))


def nt_dot(left, right):
    return lax.dot_general(
        left, right, (((1,), (1,)), ((), ())), preferred_element_type=jnp.float32
    )


def token_chunks(toks, others, x, c):
    def place(at):
        return pl.ds(pl.multiple_of(at * 256, 256), 256)

    chunks = []
    for k in range(4):
        at = 2 * ((x - k) % 4)
        chunks.append((lambda rows, k=k: toks[k][rows, :].astype(jnp.float32), place(at + c)))
        chunks.append((lambda rows, k=k: others[k, rows, :].astype(jnp.float32), place(at + 1 - c)))
    return chunks


def recurrent_kernel(where, *refs):
    toks = refs[0:4]
    others = refs[4]
    gain, conv_taps, recur_gate, input_gate, coefs, out_gains = refs[5:11]
    pieces_in = refs[11:15]
    recur_out = refs[15]
    normed, w_in, gates, acc, padded, a_s, b_s, cum_s = refs[16:]
    x, c, z, y = where[0], where[1], where[2], where[3]
    own = pl.ds(pl.multiple_of((2 * x + c) * 128, 128), 128)
    taps = conv_taps[:, own].astype(jnp.float32)
    coef = coefs[:, own]
    out_gain = out_gains[:, own]
    gates[...] = jnp.zeros(gates.shape, jnp.bfloat16)
    for d in range(2):
        for kind, ref in enumerate((recur_gate, input_gate)):
            for g in range(2):
                first = (2 * d + kind) * 128 + g * BLOCK
                gates[g * BLOCK : (g + 1) * BLOCK, first : first + BLOCK] = ref[
                    d, 2 * (2 * x + c) + g
                ]
    chunks = token_chunks(toks, others, x, c)
    length = acc.shape[0]

    def norm(i, _):
        rows = pl.ds(pl.multiple_of(i * 64, 64), 64)
        energy = None
        for load, _ in chunks:
            v = load(rows)
            e = v * v
            e = e[:, :128] + e[:, 128:]
            energy = e if energy is None else energy + e
        scale = lax.rsqrt(jnp.sum(energy, axis=1, keepdims=True) / D + EPS)
        for load, cols in chunks:
            normed[rows, cols] = (load(rows) * scale * gain[:, cols]).astype(jnp.bfloat16)
        for back_y, ref in enumerate(pieces_in):
            at = pl.ds(own_rows(z, y, i, back_y), 64)
            come = pl.multiple_of(i * 128, 128)
            w_in[at, 0:128] = ref[pl.ds(come, 64), :]
            w_in[at, 128:256] = ref[pl.ds(come + 64, 64), :]
        acc[rows, :] = jnp.zeros((64, 256), jnp.float32)
        return 0

    lax.fori_loop(0, 8, norm, 0)

    def multiply(i, _):
        at = pl.ds(pl.multiple_of(i * 256, 256), 256)
        acc[...] += jnp.dot(normed[:, at], w_in[at, :], preferred_element_type=jnp.float32)
        return 0

    lax.fori_loop(0, 8, multiply, 0)
    padded[0:8, :] = jnp.zeros((8, 128), jnp.float32)
    padded[length + 8 : length + 16, :] = jnp.zeros((8, 128), jnp.float32)

    def rounded(i, _):
        rows = pl.ds(pl.multiple_of(i * 64, 64), 64)
        v = acc[rows, 0:128].astype(jnp.bfloat16).astype(jnp.float32)
        padded[pl.ds(pl.multiple_of(i * 64 + 8, 8), 64), :] = v
        return 0

    lax.fori_loop(0, 8, rounded, 0)
    count = length // SEG

    def gated(i, _):
        near = padded[pl.ds(pl.multiple_of(i * SEG, SEG), SEG + 16), :]
        conv = taps[0:1, :] * near[6 : SEG + 6]
        for k in range(1, 4):
            conv = conv + taps[k : k + 1, :] * near[6 + k : SEG + 6 + k]
        weight = gates[...]
        high = conv.astype(jnp.bfloat16)
        rest = conv - high.astype(jnp.float32)
        mid = rest.astype(jnp.bfloat16)
        low = (rest - mid.astype(jnp.float32)).astype(jnp.bfloat16)
        mapped = (
            jnp.dot(low, weight, preferred_element_type=jnp.float32)
            + jnp.dot(mid, weight, preferred_element_type=jnp.float32)
        ) + jnp.dot(high, weight, preferred_element_type=jnp.float32)
        at = pl.ds(pl.multiple_of(i * PAD_SEG, 8), SEG)
        for d in range(2):
            rate = sigmoid(mapped[:, d * 256 : d * 256 + 128])
            inlet = sigmoid(mapped[:, d * 256 + 128 : d * 256 + 256])
            log_decay = rate * coef[d : d + 1, :]
            b_s[d, at, :] = conv * inlet * jnp.sqrt(one_minus_exp(2.0 * log_decay))
            a_s[d, at, :] = jnp.exp(log_decay)
        return 0

    lax.fori_loop(0, count, gated, 0)
    state = [jnp.zeros((count, 128), jnp.float32) for _ in range(2)]
    through = [jnp.ones((count, 128), jnp.float32) for _ in range(2)]
    for j in range(SEG):
        for d in range(2):
            at = pl.ds(j if d == 0 else SEG - 1 - j, count, stride=PAD_SEG)
            a = a_s[d, at, :]
            state[d] = a * state[d] + b_s[d, at, :]
            through[d] = a * through[d]
            b_s[d, at, :] = state[d]
            cum_s[d, at, :] = through[d]
    carries = [[None] * count for _ in range(2)]
    for d in range(2):
        order = list(range(count)) if d == 0 else list(range(count - 1, -1, -1))
        carry = jnp.zeros((1, 128), jnp.float32)
        for s in order:
            carries[d][s] = carry
            carry = through[d][s : s + 1] * carry + state[d][s : s + 1]
    for s in range(count):
        at = slice(s * PAD_SEG, s * PAD_SEG + SEG)
        rows = slice(s * SEG, s * SEG + SEG)
        summed = (b_s[0, at, :] + cum_s[0, at, :] * carries[0][s]) + (
            b_s[1, at, :] + cum_s[1, at, :] * carries[1][s]
        )
        branch_x = acc[rows, 128:256].astype(jnp.bfloat16).astype(jnp.float32)
        mixed = summed * jax.nn.gelu(branch_x, approximate=True)
        recur_out[rows, :] = (mixed * out_gain).astype(jnp.bfloat16)


def middle_kernel(where, *refs):
    toks = refs[0:4]
    tok_others = refs[4]
    recur = refs[5:9]
    recur_others = refs[9]
    weights = refs[10:14]
    weight_others = refs[14]
    post, gain = refs[15:17]
    normed, mid_own = refs[17:19]
    left, right, mid, squares = refs[19:]
    x, c, z, y = where[0], where[1], where[2], where[3]

    def place(i, _):
        at = pl.ds(own_rows(z, y, i % 8, i // 8), 64)
        come = pl.ds(pl.multiple_of(i * 64, 64), 64)
        for k in range(4):
            right[at, k * 128 : k * 128 + 128] = weights[k][come, :]
            right[at, 512 + k * 128 : 640 + k * 128] = weight_others[k, come, :]
        return 0

    lax.fori_loop(0, 32, place, 0)

    def start(i, _):
        rows = pl.ds(pl.multiple_of(i * 64, 64), 64)
        for k in range(4):
            left[rows, k * 128 : k * 128 + 128] = recur[k][rows, :]
            left[rows, 512 + k * 128 : 640 + k * 128] = recur_others[k, rows, :]
        squares[rows, :] = jnp.zeros((64, 128), jnp.float32)
        return 0

    lax.fori_loop(0, 8, start, 0)

    def multiply(i, _):
        at = pl.ds(pl.multiple_of(i * 256, 256), 256)
        total = nt_dot(left[...], right[at, :])
        mid[:, at] = total
        squares[...] += total[:, :128] * total[:, :128] + total[:, 128:] * total[:, 128:]
        return 0

    lax.fori_loop(0, 8, multiply, 0)
    chunks = token_chunks(toks, tok_others, x, c)

    def norm(i, _):
        rows = pl.ds(pl.multiple_of(i * 64, 64), 64)
        scale = lax.rsqrt(jnp.sum(squares[rows, :], axis=1, keepdims=True) / D + EPS)
        energy = None
        for n, (load, cols) in enumerate(chunks):
            v = (load(rows) + mid[rows, cols] * scale * post[:, cols]).astype(jnp.bfloat16)
            if n == 0:
                mid_own[rows, :] = v
            v = v.astype(jnp.float32)
            mid[rows, cols] = v
            e = v * v
            e = e[:, :128] + e[:, 128:]
            energy = e if energy is None else energy + e
        scale = lax.rsqrt(jnp.sum(energy, axis=1, keepdims=True) / D + EPS)
        for at in range(8):
            cols = slice(at * 256, at * 256 + 256)
            normed[rows, cols] = (mid[rows, cols] * scale * gain[:, cols]).astype(jnp.bfloat16)
        return 0

    lax.fori_loop(0, 8, norm, 0)


def forward_kernel(where, *refs):
    normed = refs[0]
    blocks = refs[1:10]
    pieces_in = refs[10:14]
    keep, send = refs[14:16]
    w_in, w_out, hidden = refs[16:]
    c, z, y = where[1], where[2], where[3]

    def place(i, _):
        for n, ref in enumerate(blocks):
            k = (0, 1, 2, 3, 4, 4, 5, 6, 7)[n]
            rows = ref.shape[0] // 8
            start = ((z - k) % 8) * 256 + (128 if n == 5 else 0) + i * rows
            come = pl.ds(pl.multiple_of(i * rows, rows), rows)
            w_in[pl.ds(pl.multiple_of(start, 16), rows), :] = ref[come, :]
        at_z = (z - i) % 8
        core, at_x = at_z % 2, at_z // 2
        come = pl.multiple_of(i * 352, 32)
        for back_y, ref in enumerate(pieces_in):
            first = pl.multiple_of(at_x * 256 + ((y - back_y) % 4) * 64, 64)
            for t in range(5):
                w_out[core, pl.ds(first, 64), t * 128 : t * 128 + 128] = ref[
                    pl.ds(come + t * 64, 64), :
                ]
            last = ref[pl.ds(come + 320, 32), :]
            w_out[core, pl.ds(first, 32), 640:704] = last[:, 0:64]
            w_out[core, pl.ds(first + 32, 32), 640:704] = last[:, 64:128]
        return 0

    lax.fori_loop(0, 8, place, 0)

    def gated(both):
        half = both.shape[1] // 2
        gate = both[:, :half]
        return (gate * sigmoid(gate) * both[:, half:]).astype(jnp.bfloat16)

    def multiply(i, _):
        at = pl.ds(pl.multiple_of(i * 256, 256), 256)
        both = jnp.dot(normed[...], w_in[:, at], preferred_element_type=jnp.float32)
        hidden[:, pl.ds(pl.multiple_of(i * 128, 128), 128)] = gated(both)
        return 0

    lax.fori_loop(0, 5, multiply, 0)
    both = jnp.dot(normed[...], w_in[:, 1280:1408], preferred_element_type=jnp.float32)
    hidden[:, 640:704] = gated(both)

    def project(i, _):
        rows = pl.ds(pl.multiple_of(i * 256, 256), 256)
        keep[i] = nt_dot(hidden[...], w_out[c, rows, :]).astype(jnp.bfloat16)
        send[i] = nt_dot(hidden[...], w_out[1 - c, rows, :]).astype(jnp.bfloat16)
        return 0

    lax.fori_loop(0, 4, project, 0)


VMEM = pl.BlockSpec(memory_space=pltpu.MemorySpace.VMEM)
SMEM = pl.BlockSpec(memory_space=pltpu.MemorySpace.SMEM)


def on_device(
    tokens,
    mixer_gain,
    recur_in,
    branch_in,
    conv_taps,
    recur_gate,
    input_gate,
    decay_param,
    recur_gain,
    recur_out,
    mixer_post,
    channel_gain,
    hidden_gate,
    hidden_up,
    hidden_down,
    channel_post,
):
    x, c = lax.axis_index("x"), lax.axis_index("c")
    rank_tp = 2 * x + c
    length, feature_width = tokens.shape
    channels = recur_in.shape[1]
    rows = recur_in.shape[0]
    width = hidden_gate.shape[1]
    where = jnp.stack([x, c, lax.axis_index("z"), lax.axis_index("y")]).astype(jnp.int32)

    narrow, wide = pl.pallas_call(
        pack_kernel,
        out_shape=(
            jax.ShapeDtypeStruct((3 * rows + width // 2, 128), jnp.bfloat16),
            jax.ShapeDtypeStruct((rows, 2 * width), jnp.bfloat16),
        ),
        in_specs=[VMEM] * 6,
        out_specs=(VMEM, VMEM),
        name="pack",
    )(recur_in, branch_in, recur_out.T, hidden_gate, hidden_up, hidden_down.T)
    out_z, in_z, down_z = pl.pallas_call(
        split_kernel,
        out_shape=(
            jax.ShapeDtypeStruct((8 * rows, 128), jnp.bfloat16),
            jax.ShapeDtypeStruct((16 * rows, 128), jnp.bfloat16),
            jax.ShapeDtypeStruct((4 * width, 128), jnp.bfloat16),
        ),
        in_specs=[VMEM] * 9,
        out_specs=(VMEM,) * 3,
        name="split",
    )(*along_z(narrow))
    wide_y = from_all_y(wide)
    hidden_y = pl.pallas_call(
        join_kernel,
        out_shape=jax.ShapeDtypeStruct((4 * rows, 2 * width), jnp.bfloat16),
        in_specs=[SMEM] + [VMEM] * 4,
        out_specs=VMEM,
        name="join",
    )(where, *wide_y)
    toks = from_all_x(tokens)
    hidden_blocks = along_z(hidden_y)
    tok_others = swap_cores(jnp.stack(toks))
    out_y = from_all_y(out_z)
    in_y = from_all_y(in_z)
    down_y = from_all_y(down_z)
    weights = pl.pallas_call(
        stack_kernel,
        out_shape=jax.ShapeDtypeStruct((D, 128), jnp.bfloat16),
        in_specs=[VMEM] * 4,
        out_specs=VMEM,
        name="stack",
    )(*out_y)
    weights = from_all_x(weights)
    weight_others = swap_cores(jnp.stack(weights))
    coef = -SHRINK * jax.nn.softplus(-decay_param)

    seg_rows = (length // SEG) * PAD_SEG
    recur_y = pl.pallas_call(
        recurrent_kernel,
        out_shape=jax.ShapeDtypeStruct((length, channels), jnp.bfloat16),
        in_specs=[SMEM] + [VMEM] * 15,
        out_specs=VMEM,
        scratch_shapes=[
            pltpu.VMEM((length, D), jnp.bfloat16),
            pltpu.VMEM((D, 256), jnp.bfloat16),
            pltpu.VMEM((channels, 4 * channels), jnp.bfloat16),
            pltpu.VMEM((length, 256), jnp.float32),
            pltpu.VMEM((length + 16, channels), jnp.float32),
            pltpu.VMEM((2, seg_rows, channels), jnp.float32),
            pltpu.VMEM((2, seg_rows, channels), jnp.float32),
            pltpu.VMEM((2, seg_rows, channels), jnp.float32),
        ],
        name="recurrent",
    )(
        where,
        *toks,
        tok_others,
        mixer_gain[None],
        conv_taps,
        recur_gate,
        input_gate,
        coef,
        recur_gain[None],
        *in_y,
    )
    recur = from_all_x(recur_y)
    recur_others = swap_cores(jnp.stack(recur))
    normed, mid_own = pl.pallas_call(
        middle_kernel,
        out_shape=(
            jax.ShapeDtypeStruct((length, D), jnp.bfloat16),
            jax.ShapeDtypeStruct((length, feature_width), jnp.bfloat16),
        ),
        in_specs=[SMEM] + [VMEM] * 17,
        out_specs=(VMEM, VMEM),
        scratch_shapes=[
            pltpu.VMEM((length, 8 * channels), jnp.bfloat16),
            pltpu.VMEM((D, 8 * channels), jnp.bfloat16),
            pltpu.VMEM((length, D), jnp.float32),
            pltpu.VMEM((length, 128), jnp.float32),
        ],
        name="middle",
    )(
        where,
        *toks,
        tok_others,
        *recur,
        recur_others,
        *weights,
        weight_others,
        mixer_post[None],
        channel_gain[None],
    )
    keep, send = pl.pallas_call(
        forward_kernel,
        out_shape=(jax.ShapeDtypeStruct((4, length, 256), jnp.bfloat16),) * 2,
        in_specs=[SMEM] + [VMEM] * 14,
        out_specs=(VMEM, VMEM),
        scratch_shapes=[
            pltpu.VMEM((D, 2 * width), jnp.bfloat16),
            pltpu.VMEM((2, D // 2, width), jnp.bfloat16),
            pltpu.VMEM((length, width), jnp.bfloat16),
        ],
        name="forward",
    )(where, normed, *hidden_blocks, *down_y)
    came = swap_cores(send)

    def pair(to):
        one = lax.dynamic_index_in_dim(keep, to, 0, False).astype(jnp.float32)
        two = lax.dynamic_index_in_dim(came, to, 0, False).astype(jnp.float32)
        return one + two

    hidden_own = pair(x)
    for k in (1, 2, 3):
        part = shift(pair((x + k) % 4).astype(jnp.bfloat16), "x", k)
        hidden_own = hidden_own + part.astype(jnp.float32)
    energy = jnp.sum(hidden_own * hidden_own, axis=1)
    everyone = jnp.broadcast_to(energy, (8, length))
    energy = jnp.sum(lax.all_to_all(everyone, TP, 0, 0, tiled=True), axis=0)
    post_own = lax.dynamic_slice_in_dim(channel_post, rank_tp * feature_width, feature_width, 0)
    return (
        mid_own.astype(jnp.float32)
        + hidden_own * lax.rsqrt(energy / D + EPS)[:, None] * post_own
    ).astype(jnp.bfloat16)


def solution(mesh):
    split = Mesh(mesh.devices.reshape(8, 4, 4, 2), ("z", "y", "x", "c"))
    placed = (
        P(FS, TP),
        P(),
        P(FS, TP),
        P(FS, TP),
        P(),
        P(),
        P(),
        P(),
        P(),
        P(TP, FS),
        P(),
        P(),
        P(FS, TP),
        P(FS, TP),
        P(TP, FS),
        P(),
    )

    return jax.shard_map(on_device, mesh=split, in_specs=placed, out_specs=P(FS, TP), check_vma=False)
```

```python
import jax
import jax.numpy as jnp
from jax import lax
from jax.experimental import pallas as pl
from jax.experimental.pallas import tpu as pltpu
from jax.sharding import Mesh
from jax.sharding import PartitionSpec as P

D = 2048
BLOCK = 64
FS = ("z", "y")
TP = ("x", "c")
EPS = 1e-06
SHRINK = 8.0
SEG = 64
PAD_SEG = 72


def shift(array, axis, by):
    n = lax.axis_size(axis)
    return lax.ppermute(array, axis, [(i, (i + by) % n) for i in range(n)])


def swap_cores(array):
    return lax.ppermute(array, "c", [(0, 1), (1, 0)])


def from_all_x(array):
    return [array] + [shift(array, "x", k) for k in (1, 2, 3)]


def from_all_y(array):
    return [array] + [shift(array, "y", k) for k in (1, 2, 3)]


def along_z(block):
    half = block.shape[0] // 2
    ahead, behind = [block], [block]
    for _ in range(3):
        ahead.append(shift(ahead[-1], "z", 1))
        behind.append(shift(behind[-1], "z", -1))
    low = shift(ahead[3][:half], "z", 1)
    high = shift(behind[3][half:], "z", -1)
    return ahead + [low, high] + behind[:0:-1]


def own_rows(z, y, back_z, back_y):
    return pl.multiple_of((((z - back_z) % 8) * 4 + (y - back_y) % 4) * 64, 64)


def pack_kernel(recur_in, branch_in, recur_out_t, gate, up, down_t, narrow, wide):
    wide[:, 0:704] = gate[...]
    wide[:, 704:1408] = up[...]
    narrow[0:64] = recur_out_t[...]
    narrow[64:128] = recur_in[...]
    narrow[128:192] = branch_in[...]
    for t in range(5):
        narrow[192 + t * 64 : 256 + t * 64] = down_t[:, t * 128 : t * 128 + 128]
    narrow[512:544, 0:64] = down_t[0:32, 640:704]
    narrow[512:544, 64:128] = down_t[32:64, 640:704]


def split_kernel(*refs):
    out, inner, down = refs[9:]
    for n, ref in enumerate(refs[:9]):
        k = (0, 1, 2, 3, 4, 4, 5, 6, 7)[n]
        if n == 4:
            out[256:320, :] = ref[0:64, :]
            inner[512:640, :] = ref[64:192, :]
            down[1408:1488, :] = ref[192:272, :]
        elif n == 5:
            down[1488:1760, :] = ref[...]
        else:
            out[k * 64 : k * 64 + 64, :] = ref[0:64, :]
            inner[k * 128 : k * 128 + 128, :] = ref[64:192, :]
            down[k * 352 : k * 352 + 352, :] = ref[192:544, :]


def stack_kernel(*refs):
    rows = refs[0].shape[0]
    for k in range(4):
        refs[4][k * rows : k * rows + rows, :] = refs[k][...]


def sigmoid(v):
    return 1.0 / (1.0 + jnp.exp(-v))


def one_minus_exp(v):
    series = jnp.ones_like(v)
    for n in range(9, 1, -1):
        series = 1.0 + v * (1.0 / n) * series
    return jnp.where(v > -0.5, -v * series, 1.0 - jnp.exp(v))


def nt_dot(left, right):
    return lax.dot_general(
        left, right, (((1,), (1,)), ((), ())), preferred_element_type=jnp.float32
    )


def recurrent_kernel(where, *refs):
    toks = refs[0:4]
    others = refs[4]
    gain, conv_taps, recur_gate, input_gate, coefs, out_gains = refs[5:11]
    pieces_in = refs[11:15]
    recur_out = refs[15]
    normed, w_in, gates, padded, a_s, b_s, cum_s = refs[16:]
    x, c, z, y = where[0], where[1], where[2], where[3]
    own = pl.ds(pl.multiple_of((2 * x + c) * 128, 128), 128)
    taps = conv_taps[:, own].astype(jnp.float32)
    coef = coefs[:, own]
    out_gain = out_gains[:, own]
    gates[...] = jnp.zeros(gates.shape, jnp.bfloat16)
    for d in range(2):
        for kind, ref in enumerate((recur_gate, input_gate)):
            for g in range(2):
                first = (2 * d + kind) * 128 + g * BLOCK
                gates[g * BLOCK : (g + 1) * BLOCK, first : first + BLOCK] = ref[
                    d, 2 * (2 * x + c) + g
                ]
    chunks = [(toks[k], 2 * ((x - k) % 4) + c) for k in range(4)]
    chunks += [(others.at[k], 2 * ((x - k) % 4) + 1 - c) for k in range(4)]
    energy = None
    for ref, _ in chunks:
        v = ref[...].astype(jnp.float32)
        e = jnp.sum(v * v, axis=1, keepdims=True)
        energy = e if energy is None else energy + e
    scale = lax.rsqrt(energy / D + EPS)
    for ref, at in chunks:
        cols = pl.ds(pl.multiple_of(at * 256, 256), 256)
        v = ref[...].astype(jnp.float32)
        normed[:, cols] = (v * scale * gain[:, cols]).astype(jnp.bfloat16)
    for back_y, ref in enumerate(pieces_in):
        for back_z in range(8):
            at = pl.ds(own_rows(z, y, back_z, back_y), 64)
            w_in[at, 0:128] = ref[back_z * 128 : back_z * 128 + 64, :]
            w_in[at, 128:256] = ref[back_z * 128 + 64 : back_z * 128 + 128, :]
    both = jnp.dot(normed[...], w_in[...], preferred_element_type=jnp.float32)
    recur_x = both[:, 0:128].astype(jnp.bfloat16).astype(jnp.float32)
    branch_x = both[:, 128:256].astype(jnp.bfloat16).astype(jnp.float32)
    length = recur_x.shape[0]
    padded[0:8, :] = jnp.zeros((8, 128), jnp.float32)
    padded[length + 8 : length + 16, :] = jnp.zeros((8, 128), jnp.float32)
    padded[8 : length + 8, :] = recur_x
    conv = taps[0:1, :] * padded[6 : length + 6, :]
    for k in range(1, 4):
        conv = conv + taps[k : k + 1, :] * padded[6 + k : length + 6 + k, :]
    weight = gates[...]
    high = conv.astype(jnp.bfloat16)
    rest = conv - high.astype(jnp.float32)
    mid = rest.astype(jnp.bfloat16)
    low = (rest - mid.astype(jnp.float32)).astype(jnp.bfloat16)
    mapped = (
        jnp.dot(low, weight, preferred_element_type=jnp.float32)
        + jnp.dot(mid, weight, preferred_element_type=jnp.float32)
    ) + jnp.dot(high, weight, preferred_element_type=jnp.float32)
    count = length // SEG
    for d in range(2):
        rate = sigmoid(mapped[:, d * 256 : d * 256 + 128])
        inlet = sigmoid(mapped[:, d * 256 + 128 : d * 256 + 256])
        log_decay = rate * coef[d : d + 1, :]
        inflow = conv * inlet * jnp.sqrt(one_minus_exp(2.0 * log_decay))
        decay = jnp.exp(log_decay)
        for s in range(count):
            a_s[d, s * PAD_SEG : s * PAD_SEG + SEG, :] = decay[s * SEG : s * SEG + SEG]
            b_s[d, s * PAD_SEG : s * PAD_SEG + SEG, :] = inflow[s * SEG : s * SEG + SEG]
    state = [jnp.zeros((count, 128), jnp.float32) for _ in range(2)]
    through = [jnp.ones((count, 128), jnp.float32) for _ in range(2)]
    for j in range(SEG):
        for d in range(2):
            at = pl.ds(j if d == 0 else SEG - 1 - j, count, stride=PAD_SEG)
            a = a_s[d, at, :]
            state[d] = a * state[d] + b_s[d, at, :]
            through[d] = a * through[d]
            b_s[d, at, :] = state[d]
            cum_s[d, at, :] = through[d]
    carries = [[None] * count for _ in range(2)]
    for d in range(2):
        order = list(range(count)) if d == 0 else list(range(count - 1, -1, -1))
        carry = jnp.zeros((1, 128), jnp.float32)
        for s in order:
            carries[d][s] = carry
            carry = through[d][s : s + 1] * carry + state[d][s : s + 1]
    summed = []
    for s in range(count):
        at = slice(s * PAD_SEG, s * PAD_SEG + SEG)
        summed.append(
            (b_s[0, at, :] + cum_s[0, at, :] * carries[0][s])
            + (b_s[1, at, :] + cum_s[1, at, :] * carries[1][s])
        )
    mixed = jnp.concatenate(summed, axis=0) * jax.nn.gelu(branch_x, approximate=True)
    recur_out[...] = (mixed * out_gain).astype(jnp.bfloat16)


def middle_kernel(where, *refs):
    toks = refs[0:4]
    tok_others = refs[4]
    recur = refs[5:9]
    recur_others = refs[9]
    weights = refs[10:14]
    weight_others = refs[14]
    post, gain = refs[15:17]
    normed, mid_own = refs[17:19]
    left, right, mid = refs[19:]
    x, c, z, y = where[0], where[1], where[2], where[3]
    for k in range(4):
        left[:, k * 128 : k * 128 + 128] = recur[k][...]
        left[:, 512 + k * 128 : 640 + k * 128] = recur_others[k]
        for back_y in range(4):
            for back_z in range(8):
                at = pl.ds(own_rows(z, y, back_z, back_y), 64)
                come = slice((back_y * 8 + back_z) * 64, (back_y * 8 + back_z) * 64 + 64)
                right[at, k * 128 : k * 128 + 128] = weights[k][come, :]
                right[at, 512 + k * 128 : 640 + k * 128] = weight_others[k, come, :]
    total = nt_dot(left[...], right[...])
    scale = lax.rsqrt(jnp.sum(total * total, axis=1, keepdims=True) / D + EPS)
    mid[...] = total * scale * post[...]
    chunks = [(toks[k], 2 * ((x - k) % 4) + c) for k in range(4)]
    chunks += [(tok_others.at[k], 2 * ((x - k) % 4) + 1 - c) for k in range(4)]
    energy = None
    for tok, at in chunks:
        cols = pl.ds(pl.multiple_of(at * 256, 256), 256)
        v = (tok[...].astype(jnp.float32) + mid[:, cols]).astype(jnp.bfloat16)
        if tok is toks[0]:
            mid_own[...] = v
        v = v.astype(jnp.float32)
        mid[:, cols] = v
        e = jnp.sum(v * v, axis=1, keepdims=True)
        energy = e if energy is None else energy + e
    scale = lax.rsqrt(energy / D + EPS)
    for at in range(8):
        cols = slice(at * 256, at * 256 + 256)
        normed[:, cols] = (mid[:, cols] * scale * gain[:, cols]).astype(jnp.bfloat16)


def forward_kernel(where, normed, w_in, *refs):
    pieces_in = refs[0:4]
    keep, send = refs[4:6]
    w_out = refs[6]
    c, z, y = where[1], where[2], where[3]
    for back_z in range(8):
        at_z = (z - back_z) % 8
        core, at_x = at_z % 2, at_z // 2
        for back_y, ref in enumerate(pieces_in):
            first = pl.multiple_of(at_x * 256 + ((y - back_y) % 4) * 64, 64)
            come = back_z * 352
            for t in range(5):
                w_out[core, pl.ds(first, 64), t * 128 : t * 128 + 128] = ref[
                    come + t * 64 : come + t * 64 + 64, :
                ]
            last = ref[come + 320 : come + 352, :]
            w_out[core, pl.ds(first, 32), 640:704] = last[:, 0:64]
            w_out[core, pl.ds(first + 32, 32), 640:704] = last[:, 64:128]
    both = jnp.dot(normed[...], w_in[...], preferred_element_type=jnp.float32)
    width = both.shape[1] // 2
    gate = both[:, :width]
    hidden = (gate * sigmoid(gate) * both[:, width:]).astype(jnp.bfloat16)
    for to in range(4):
        rows = slice(to * 256, to * 256 + 256)
        send[to] = nt_dot(hidden, w_out[1 - c, rows, :]).astype(jnp.bfloat16)
        keep[to] = nt_dot(hidden, w_out[c, rows, :]).astype(jnp.bfloat16)


VMEM = pl.BlockSpec(memory_space=pltpu.MemorySpace.VMEM)
SMEM = pl.BlockSpec(memory_space=pltpu.MemorySpace.SMEM)


def on_device(
    tokens,
    mixer_gain,
    recur_in,
    branch_in,
    conv_taps,
    recur_gate,
    input_gate,
    decay_param,
    recur_gain,
    recur_out,
    mixer_post,
    channel_gain,
    hidden_gate,
    hidden_up,
    hidden_down,
    channel_post,
):
    x, c = lax.axis_index("x"), lax.axis_index("c")
    rank_tp = 2 * x + c
    length, feature_width = tokens.shape
    channels = recur_in.shape[1]
    rows = recur_in.shape[0]
    width = hidden_gate.shape[1]
    where = jnp.stack([x, c, lax.axis_index("z"), lax.axis_index("y")]).astype(jnp.int32)

    narrow, wide = pl.pallas_call(
        pack_kernel,
        out_shape=(
            jax.ShapeDtypeStruct((3 * rows + width // 2, 128), jnp.bfloat16),
            jax.ShapeDtypeStruct((rows, 2 * width), jnp.bfloat16),
        ),
        in_specs=[VMEM] * 6,
        out_specs=(VMEM, VMEM),
        name="pack",
    )(recur_in, branch_in, recur_out.T, hidden_gate, hidden_up, hidden_down.T)
    out_z, in_z, down_z = pl.pallas_call(
        split_kernel,
        out_shape=(
            jax.ShapeDtypeStruct((8 * rows, 128), jnp.bfloat16),
            jax.ShapeDtypeStruct((16 * rows, 128), jnp.bfloat16),
            jax.ShapeDtypeStruct((4 * width, 128), jnp.bfloat16),
        ),
        in_specs=[VMEM] * 9,
        out_specs=(VMEM,) * 3,
        name="split",
    )(*along_z(narrow))
    hidden_all = lax.all_gather(wide, FS, axis=0, tiled=True)
    toks = from_all_x(tokens)
    tok_others = swap_cores(jnp.stack(toks))
    out_y = from_all_y(out_z)
    in_y = from_all_y(in_z)
    down_y = from_all_y(down_z)
    weights = pl.pallas_call(
        stack_kernel,
        out_shape=jax.ShapeDtypeStruct((D, 128), jnp.bfloat16),
        in_specs=[VMEM] * 4,
        out_specs=VMEM,
        name="stack",
    )(*out_y)
    weights = from_all_x(weights)
    weight_others = swap_cores(jnp.stack(weights))
    coef = -SHRINK * jax.nn.softplus(-decay_param)

    seg_rows = (length // SEG) * PAD_SEG
    recur_y = pl.pallas_call(
        recurrent_kernel,
        out_shape=jax.ShapeDtypeStruct((length, channels), jnp.bfloat16),
        in_specs=[SMEM] + [VMEM] * 15,
        out_specs=VMEM,
        scratch_shapes=[
            pltpu.VMEM((length, D), jnp.bfloat16),
            pltpu.VMEM((D, 256), jnp.bfloat16),
            pltpu.VMEM((channels, 4 * channels), jnp.bfloat16),
            pltpu.VMEM((length + 16, channels), jnp.float32),
            pltpu.VMEM((2, seg_rows, channels), jnp.float32),
            pltpu.VMEM((2, seg_rows, channels), jnp.float32),
            pltpu.VMEM((2, seg_rows, channels), jnp.float32),
        ],
        name="recurrent",
    )(
        where,
        *toks,
        tok_others,
        mixer_gain[None],
        conv_taps,
        recur_gate,
        input_gate,
        coef,
        recur_gain[None],
        *in_y,
    )
    recur = from_all_x(recur_y)
    recur_others = swap_cores(jnp.stack(recur))
    normed, mid_own = pl.pallas_call(
        middle_kernel,
        out_shape=(
            jax.ShapeDtypeStruct((length, D), jnp.bfloat16),
            jax.ShapeDtypeStruct((length, feature_width), jnp.bfloat16),
        ),
        in_specs=[SMEM] + [VMEM] * 17,
        out_specs=(VMEM, VMEM),
        scratch_shapes=[
            pltpu.VMEM((length, 8 * channels), jnp.bfloat16),
            pltpu.VMEM((D, 8 * channels), jnp.bfloat16),
            pltpu.VMEM((length, D), jnp.float32),
        ],
        name="middle",
    )(
        where,
        *toks,
        tok_others,
        *recur,
        recur_others,
        *weights,
        weight_others,
        mixer_post[None],
        channel_gain[None],
    )
    keep, send = pl.pallas_call(
        forward_kernel,
        out_shape=(jax.ShapeDtypeStruct((4, length, 256), jnp.bfloat16),) * 2,
        in_specs=[SMEM] + [VMEM] * 6,
        out_specs=(VMEM, VMEM),
        scratch_shapes=[
            pltpu.VMEM((2, D // 2, width), jnp.bfloat16),
        ],
        name="forward",
    )(where, normed, hidden_all, *down_y)
    came = swap_cores(send)

    def pair(to):
        one = lax.dynamic_index_in_dim(keep, to, 0, False).astype(jnp.float32)
        two = lax.dynamic_index_in_dim(came, to, 0, False).astype(jnp.float32)
        return one + two

    hidden_own = pair(x)
    for k in (1, 2, 3):
        part = shift(pair((x + k) % 4).astype(jnp.bfloat16), "x", k)
        hidden_own = hidden_own + part.astype(jnp.float32)
    energy = jnp.sum(hidden_own * hidden_own, axis=1)
    everyone = jnp.broadcast_to(energy, (8, length))
    energy = jnp.sum(lax.all_to_all(everyone, TP, 0, 0, tiled=True), axis=0)
    post_own = lax.dynamic_slice_in_dim(channel_post, rank_tp * feature_width, feature_width, 0)
    return (
        mid_own.astype(jnp.float32)
        + hidden_own * lax.rsqrt(energy / D + EPS)[:, None] * post_own
    ).astype(jnp.bfloat16)


def solution(mesh):
    split = Mesh(mesh.devices.reshape(8, 4, 4, 2), ("z", "y", "x", "c"))
    placed = (
        P(FS, TP),
        P(),
        P(FS, TP),
        P(FS, TP),
        P(),
        P(),
        P(),
        P(),
        P(),
        P(TP, FS),
        P(),
        P(),
        P(FS, TP),
        P(FS, TP),
        P(TP, FS),
        P(),
    )

    return jax.shard_map(on_device, mesh=split, in_specs=placed, out_specs=P(FS, TP), check_vma=False)
```

```python
import jax
import jax.numpy as jnp
from jax import lax
from jax.experimental import pallas as pl
from jax.experimental.pallas import tpu as pltpu
from jax.sharding import Mesh
from jax.sharding import PartitionSpec as P

D = 2048
BLOCK = 64
FS = ("z", "y")
TP = ("x", "c")
EPS = 1e-06
SHRINK = 8.0
SEG = 64
PAD_SEG = 72


def shift(array, axis, by):
    n = lax.axis_size(axis)
    return lax.ppermute(array, axis, [(i, (i + by) % n) for i in range(n)])


def swap_cores(array):
    return lax.ppermute(array, "c", [(0, 1), (1, 0)])


def from_all_x(array):
    return [array] + [shift(array, "x", k) for k in (1, 2, 3)]


def from_all_y(array):
    return [array] + [shift(array, "y", k) for k in (1, 2, 3)]


def along_z(block):
    half = block.shape[0] // 2
    ahead, behind = [block], [block]
    for _ in range(3):
        ahead.append(shift(ahead[-1], "z", 1))
        behind.append(shift(behind[-1], "z", -1))
    low = shift(ahead[3][:half], "z", 1)
    high = shift(behind[3][half:], "z", -1)
    return ahead + [low, high] + behind[:0:-1]


def own_rows(z, y, back_z, back_y):
    return pl.multiple_of((((z - back_z) % 8) * 4 + (y - back_y) % 4) * 64, 64)


def pack_kernel(recur_in, branch_in, recur_out_t, gate, up, down_t, narrow, wide):
    wide[:, 0:704] = gate[...]
    wide[:, 704:1408] = up[...]
    narrow[0:64] = recur_out_t[...]
    narrow[64:128] = recur_in[...]
    narrow[128:192] = branch_in[...]
    for t in range(5):
        narrow[192 + t * 64 : 256 + t * 64] = down_t[:, t * 128 : t * 128 + 128]
    narrow[512:544, 0:64] = down_t[0:32, 640:704]
    narrow[512:544, 64:128] = down_t[32:64, 640:704]


def split_kernel(*refs):
    out, inner, down = refs[9:]
    for n, ref in enumerate(refs[:9]):
        k = (0, 1, 2, 3, 4, 4, 5, 6, 7)[n]
        if n == 4:
            out[256:320, :] = ref[0:64, :]
            inner[512:640, :] = ref[64:192, :]
            down[1408:1488, :] = ref[192:272, :]
        elif n == 5:
            down[1488:1760, :] = ref[...]
        else:
            out[k * 64 : k * 64 + 64, :] = ref[0:64, :]
            inner[k * 128 : k * 128 + 128, :] = ref[64:192, :]
            down[k * 352 : k * 352 + 352, :] = ref[192:544, :]


def stack_kernel(*refs):
    rows = refs[0].shape[0]
    for k in range(4):
        refs[4][k * rows : k * rows + rows, :] = refs[k][...]


def join_kernel(where, *refs):
    y = where[3]
    for k in range(4):
        refs[4][pl.ds(pl.multiple_of(((y - k) % 4) * 64, 64), 64), :] = refs[k][...]


def sigmoid(v):
    return 1.0 / (1.0 + jnp.exp(-v))


def one_minus_exp(v):
    series = jnp.ones_like(v)
    for n in range(9, 1, -1):
        series = 1.0 + v * (1.0 / n) * series
    return jnp.where(v > -0.5, -v * series, 1.0 - jnp.exp(v))


def nt_dot(left, right):
    return lax.dot_general(
        left, right, (((1,), (1,)), ((), ())), preferred_element_type=jnp.float32
    )


def recurrent_kernel(where, *refs):
    toks = refs[0:4]
    others = refs[4]
    gain, conv_taps, recur_gate, input_gate, coefs, out_gains = refs[5:11]
    pieces_in = refs[11:15]
    recur_out = refs[15]
    normed, w_in, gates, padded, a_s, b_s, cum_s = refs[16:]
    x, c, z, y = where[0], where[1], where[2], where[3]
    own = pl.ds(pl.multiple_of((2 * x + c) * 128, 128), 128)
    taps = conv_taps[:, own].astype(jnp.float32)
    coef = coefs[:, own]
    out_gain = out_gains[:, own]
    gates[...] = jnp.zeros(gates.shape, jnp.bfloat16)
    for d in range(2):
        for kind, ref in enumerate((recur_gate, input_gate)):
            for g in range(2):
                first = (2 * d + kind) * 128 + g * BLOCK
                gates[g * BLOCK : (g + 1) * BLOCK, first : first + BLOCK] = ref[
                    d, 2 * (2 * x + c) + g
                ]
    chunks = [(toks[k], 2 * ((x - k) % 4) + c) for k in range(4)]
    chunks += [(others.at[k], 2 * ((x - k) % 4) + 1 - c) for k in range(4)]
    energy = None
    for ref, _ in chunks:
        v = ref[...].astype(jnp.float32)
        e = jnp.sum(v * v, axis=1, keepdims=True)
        energy = e if energy is None else energy + e
    scale = lax.rsqrt(energy / D + EPS)
    for ref, at in chunks:
        cols = pl.ds(pl.multiple_of(at * 256, 256), 256)
        v = ref[...].astype(jnp.float32)
        normed[:, cols] = (v * scale * gain[:, cols]).astype(jnp.bfloat16)
    for back_y, ref in enumerate(pieces_in):
        for back_z in range(8):
            at = pl.ds(own_rows(z, y, back_z, back_y), 64)
            w_in[at, 0:128] = ref[back_z * 128 : back_z * 128 + 64, :]
            w_in[at, 128:256] = ref[back_z * 128 + 64 : back_z * 128 + 128, :]
    both = jnp.dot(normed[...], w_in[...], preferred_element_type=jnp.float32)
    recur_x = both[:, 0:128].astype(jnp.bfloat16).astype(jnp.float32)
    branch_x = both[:, 128:256].astype(jnp.bfloat16).astype(jnp.float32)
    length = recur_x.shape[0]
    padded[0:8, :] = jnp.zeros((8, 128), jnp.float32)
    padded[length + 8 : length + 16, :] = jnp.zeros((8, 128), jnp.float32)
    padded[8 : length + 8, :] = recur_x
    conv = taps[0:1, :] * padded[6 : length + 6, :]
    for k in range(1, 4):
        conv = conv + taps[k : k + 1, :] * padded[6 + k : length + 6 + k, :]
    weight = gates[...]
    high = conv.astype(jnp.bfloat16)
    rest = conv - high.astype(jnp.float32)
    mid = rest.astype(jnp.bfloat16)
    low = (rest - mid.astype(jnp.float32)).astype(jnp.bfloat16)
    mapped = (
        jnp.dot(low, weight, preferred_element_type=jnp.float32)
        + jnp.dot(mid, weight, preferred_element_type=jnp.float32)
    ) + jnp.dot(high, weight, preferred_element_type=jnp.float32)
    count = length // SEG
    for d in range(2):
        rate = sigmoid(mapped[:, d * 256 : d * 256 + 128])
        inlet = sigmoid(mapped[:, d * 256 + 128 : d * 256 + 256])
        log_decay = rate * coef[d : d + 1, :]
        inflow = conv * inlet * jnp.sqrt(one_minus_exp(2.0 * log_decay))
        decay = jnp.exp(log_decay)
        for s in range(count):
            a_s[d, s * PAD_SEG : s * PAD_SEG + SEG, :] = decay[s * SEG : s * SEG + SEG]
            b_s[d, s * PAD_SEG : s * PAD_SEG + SEG, :] = inflow[s * SEG : s * SEG + SEG]
    state = [jnp.zeros((count, 128), jnp.float32) for _ in range(2)]
    through = [jnp.ones((count, 128), jnp.float32) for _ in range(2)]
    for j in range(SEG):
        for d in range(2):
            at = pl.ds(j if d == 0 else SEG - 1 - j, count, stride=PAD_SEG)
            a = a_s[d, at, :]
            state[d] = a * state[d] + b_s[d, at, :]
            through[d] = a * through[d]
            b_s[d, at, :] = state[d]
            cum_s[d, at, :] = through[d]
    carries = [[None] * count for _ in range(2)]
    for d in range(2):
        order = list(range(count)) if d == 0 else list(range(count - 1, -1, -1))
        carry = jnp.zeros((1, 128), jnp.float32)
        for s in order:
            carries[d][s] = carry
            carry = through[d][s : s + 1] * carry + state[d][s : s + 1]
    summed = []
    for s in range(count):
        at = slice(s * PAD_SEG, s * PAD_SEG + SEG)
        summed.append(
            (b_s[0, at, :] + cum_s[0, at, :] * carries[0][s])
            + (b_s[1, at, :] + cum_s[1, at, :] * carries[1][s])
        )
    mixed = jnp.concatenate(summed, axis=0) * jax.nn.gelu(branch_x, approximate=True)
    recur_out[...] = (mixed * out_gain).astype(jnp.bfloat16)


def middle_kernel(where, *refs):
    toks = refs[0:4]
    tok_others = refs[4]
    recur = refs[5:9]
    recur_others = refs[9]
    weights = refs[10:14]
    weight_others = refs[14]
    post, gain = refs[15:17]
    normed, mid_own = refs[17:19]
    left, right, mid = refs[19:]
    x, c, z, y = where[0], where[1], where[2], where[3]
    for k in range(4):
        left[:, k * 128 : k * 128 + 128] = recur[k][...]
        left[:, 512 + k * 128 : 640 + k * 128] = recur_others[k]
        for back_y in range(4):
            for back_z in range(8):
                at = pl.ds(own_rows(z, y, back_z, back_y), 64)
                come = slice((back_y * 8 + back_z) * 64, (back_y * 8 + back_z) * 64 + 64)
                right[at, k * 128 : k * 128 + 128] = weights[k][come, :]
                right[at, 512 + k * 128 : 640 + k * 128] = weight_others[k, come, :]
    total = nt_dot(left[...], right[...])
    scale = lax.rsqrt(jnp.sum(total * total, axis=1, keepdims=True) / D + EPS)
    mid[...] = total * scale * post[...]
    chunks = [(toks[k], 2 * ((x - k) % 4) + c) for k in range(4)]
    chunks += [(tok_others.at[k], 2 * ((x - k) % 4) + 1 - c) for k in range(4)]
    energy = None
    for tok, at in chunks:
        cols = pl.ds(pl.multiple_of(at * 256, 256), 256)
        v = (tok[...].astype(jnp.float32) + mid[:, cols]).astype(jnp.bfloat16)
        if tok is toks[0]:
            mid_own[...] = v
        v = v.astype(jnp.float32)
        mid[:, cols] = v
        e = jnp.sum(v * v, axis=1, keepdims=True)
        energy = e if energy is None else energy + e
    scale = lax.rsqrt(energy / D + EPS)
    for at in range(8):
        cols = slice(at * 256, at * 256 + 256)
        normed[:, cols] = (mid[:, cols] * scale * gain[:, cols]).astype(jnp.bfloat16)


def forward_kernel(where, normed, *refs):
    blocks = refs[0:9]
    pieces_in = refs[9:13]
    keep, send = refs[13:15]
    w_in, w_out = refs[15:]
    c, z, y = where[1], where[2], where[3]
    for n, ref in enumerate(blocks):
        k = (0, 1, 2, 3, 4, 4, 5, 6, 7)[n]
        start = ((z - k) % 8) * 256 + (128 if n == 5 else 0)
        w_in[pl.ds(pl.multiple_of(start, 128), ref.shape[0]), :] = ref[...]
    for back_z in range(8):
        at_z = (z - back_z) % 8
        core, at_x = at_z % 2, at_z // 2
        for back_y, ref in enumerate(pieces_in):
            first = pl.multiple_of(at_x * 256 + ((y - back_y) % 4) * 64, 64)
            come = back_z * 352
            for t in range(5):
                w_out[core, pl.ds(first, 64), t * 128 : t * 128 + 128] = ref[
                    come + t * 64 : come + t * 64 + 64, :
                ]
            last = ref[come + 320 : come + 352, :]
            w_out[core, pl.ds(first, 32), 640:704] = last[:, 0:64]
            w_out[core, pl.ds(first + 32, 32), 640:704] = last[:, 64:128]
    both = jnp.dot(normed[...], w_in[...], preferred_element_type=jnp.float32)
    width = both.shape[1] // 2
    gate = both[:, :width]
    hidden = (gate * sigmoid(gate) * both[:, width:]).astype(jnp.bfloat16)
    for to in range(4):
        rows = slice(to * 256, to * 256 + 256)
        send[to] = nt_dot(hidden, w_out[1 - c, rows, :]).astype(jnp.bfloat16)
        keep[to] = nt_dot(hidden, w_out[c, rows, :]).astype(jnp.bfloat16)


VMEM = pl.BlockSpec(memory_space=pltpu.MemorySpace.VMEM)
SMEM = pl.BlockSpec(memory_space=pltpu.MemorySpace.SMEM)


def on_device(
    tokens,
    mixer_gain,
    recur_in,
    branch_in,
    conv_taps,
    recur_gate,
    input_gate,
    decay_param,
    recur_gain,
    recur_out,
    mixer_post,
    channel_gain,
    hidden_gate,
    hidden_up,
    hidden_down,
    channel_post,
):
    x, c = lax.axis_index("x"), lax.axis_index("c")
    rank_tp = 2 * x + c
    length, feature_width = tokens.shape
    channels = recur_in.shape[1]
    rows = recur_in.shape[0]
    width = hidden_gate.shape[1]
    where = jnp.stack([x, c, lax.axis_index("z"), lax.axis_index("y")]).astype(jnp.int32)

    narrow, wide = pl.pallas_call(
        pack_kernel,
        out_shape=(
            jax.ShapeDtypeStruct((3 * rows + width // 2, 128), jnp.bfloat16),
            jax.ShapeDtypeStruct((rows, 2 * width), jnp.bfloat16),
        ),
        in_specs=[VMEM] * 6,
        out_specs=(VMEM, VMEM),
        name="pack",
    )(recur_in, branch_in, recur_out.T, hidden_gate, hidden_up, hidden_down.T)
    out_z, in_z, down_z = pl.pallas_call(
        split_kernel,
        out_shape=(
            jax.ShapeDtypeStruct((8 * rows, 128), jnp.bfloat16),
            jax.ShapeDtypeStruct((16 * rows, 128), jnp.bfloat16),
            jax.ShapeDtypeStruct((4 * width, 128), jnp.bfloat16),
        ),
        in_specs=[VMEM] * 9,
        out_specs=(VMEM,) * 3,
        name="split",
    )(*along_z(narrow))
    wide_y = from_all_y(wide)
    hidden_y = pl.pallas_call(
        join_kernel,
        out_shape=jax.ShapeDtypeStruct((4 * rows, 2 * width), jnp.bfloat16),
        in_specs=[SMEM] + [VMEM] * 4,
        out_specs=VMEM,
        name="join",
    )(where, *wide_y)
    toks = from_all_x(tokens)
    hidden_blocks = along_z(hidden_y)
    tok_others = swap_cores(jnp.stack(toks))
    out_y = from_all_y(out_z)
    in_y = from_all_y(in_z)
    down_y = from_all_y(down_z)
    weights = pl.pallas_call(
        stack_kernel,
        out_shape=jax.ShapeDtypeStruct((D, 128), jnp.bfloat16),
        in_specs=[VMEM] * 4,
        out_specs=VMEM,
        name="stack",
    )(*out_y)
    weights = from_all_x(weights)
    weight_others = swap_cores(jnp.stack(weights))
    coef = -SHRINK * jax.nn.softplus(-decay_param)

    seg_rows = (length // SEG) * PAD_SEG
    recur_y = pl.pallas_call(
        recurrent_kernel,
        out_shape=jax.ShapeDtypeStruct((length, channels), jnp.bfloat16),
        in_specs=[SMEM] + [VMEM] * 15,
        out_specs=VMEM,
        scratch_shapes=[
            pltpu.VMEM((length, D), jnp.bfloat16),
            pltpu.VMEM((D, 256), jnp.bfloat16),
            pltpu.VMEM((channels, 4 * channels), jnp.bfloat16),
            pltpu.VMEM((length + 16, channels), jnp.float32),
            pltpu.VMEM((2, seg_rows, channels), jnp.float32),
            pltpu.VMEM((2, seg_rows, channels), jnp.float32),
            pltpu.VMEM((2, seg_rows, channels), jnp.float32),
        ],
        name="recurrent",
    )(
        where,
        *toks,
        tok_others,
        mixer_gain[None],
        conv_taps,
        recur_gate,
        input_gate,
        coef,
        recur_gain[None],
        *in_y,
    )
    recur = from_all_x(recur_y)
    recur_others = swap_cores(jnp.stack(recur))
    normed, mid_own = pl.pallas_call(
        middle_kernel,
        out_shape=(
            jax.ShapeDtypeStruct((length, D), jnp.bfloat16),
            jax.ShapeDtypeStruct((length, feature_width), jnp.bfloat16),
        ),
        in_specs=[SMEM] + [VMEM] * 17,
        out_specs=(VMEM, VMEM),
        scratch_shapes=[
            pltpu.VMEM((length, 8 * channels), jnp.bfloat16),
            pltpu.VMEM((D, 8 * channels), jnp.bfloat16),
            pltpu.VMEM((length, D), jnp.float32),
        ],
        name="middle",
    )(
        where,
        *toks,
        tok_others,
        *recur,
        recur_others,
        *weights,
        weight_others,
        mixer_post[None],
        channel_gain[None],
    )
    keep, send = pl.pallas_call(
        forward_kernel,
        out_shape=(jax.ShapeDtypeStruct((4, length, 256), jnp.bfloat16),) * 2,
        in_specs=[SMEM] + [VMEM] * 14,
        out_specs=(VMEM, VMEM),
        scratch_shapes=[
            pltpu.VMEM((D, 2 * width), jnp.bfloat16),
            pltpu.VMEM((2, D // 2, width), jnp.bfloat16),
        ],
        name="forward",
    )(where, normed, *hidden_blocks, *down_y)
    came = swap_cores(send)

    def pair(to):
        one = lax.dynamic_index_in_dim(keep, to, 0, False).astype(jnp.float32)
        two = lax.dynamic_index_in_dim(came, to, 0, False).astype(jnp.float32)
        return one + two

    hidden_own = pair(x)
    for k in (1, 2, 3):
        part = shift(pair((x + k) % 4).astype(jnp.bfloat16), "x", k)
        hidden_own = hidden_own + part.astype(jnp.float32)
    energy = jnp.sum(hidden_own * hidden_own, axis=1)
    everyone = jnp.broadcast_to(energy, (8, length))
    energy = jnp.sum(lax.all_to_all(everyone, TP, 0, 0, tiled=True), axis=0)
    post_own = lax.dynamic_slice_in_dim(channel_post, rank_tp * feature_width, feature_width, 0)
    return (
        mid_own.astype(jnp.float32)
        + hidden_own * lax.rsqrt(energy / D + EPS)[:, None] * post_own
    ).astype(jnp.bfloat16)


def solution(mesh):
    split = Mesh(mesh.devices.reshape(8, 4, 4, 2), ("z", "y", "x", "c"))
    placed = (
        P(FS, TP),
        P(),
        P(FS, TP),
        P(FS, TP),
        P(),
        P(),
        P(),
        P(),
        P(),
        P(TP, FS),
        P(),
        P(),
        P(FS, TP),
        P(FS, TP),
        P(TP, FS),
        P(),
    )

    return jax.shard_map(on_device, mesh=split, in_specs=placed, out_specs=P(FS, TP), check_vma=False)
```

```python
import jax
import jax.numpy as jnp
from jax import lax
from jax.experimental import pallas as pl
from jax.experimental.pallas import tpu as pltpu
from jax.sharding import Mesh
from jax.sharding import PartitionSpec as P

D = 2048
BLOCK = 64
FS = ("z", "y")
TP = ("x", "c")
EPS = 1e-06
SHRINK = 8.0
SEG = 64
PAD_SEG = 72


def shift(array, axis, by):
    n = lax.axis_size(axis)
    return lax.ppermute(array, axis, [(i, (i + by) % n) for i in range(n)])


def swap_cores(array):
    return lax.ppermute(array, "c", [(0, 1), (1, 0)])


def from_all_x(array):
    return [array] + [shift(array, "x", k) for k in (1, 2, 3)]


def from_all_y(array):
    return [array] + [shift(array, "y", k) for k in (1, 2, 3)]


def along_z(block):
    ahead, behind = [block], [block]
    for _ in range(3):
        ahead.append(shift(ahead[-1], "z", 1))
        behind.append(shift(behind[-1], "z", -1))
    passed = jnp.where(lax.axis_index("c") == 0, ahead[3], behind[3])
    n = lax.axis_size("z")
    pairs = [(2 * i, 2 * ((i + 1) % n)) for i in range(n)]
    pairs += [(2 * i + 1, 2 * ((i - 1) % n) + 1) for i in range(n)]
    last = lax.ppermute(passed, ("z", "c"), pairs)
    return ahead + [last] + behind[:0:-1]


def copied(plan, arrays, rows):
    width = arrays[0].shape[1]

    def kernel(*refs):
        sems = refs[-1]
        copies = [
            pltpu.make_async_copy(
                refs[a].at[pl.ds(first, n)],
                refs[len(arrays) + b].at[pl.ds(to, n)],
                sems.at[m],
            )
            for m, (a, first, b, to, n) in enumerate(plan)
        ]
        for copy in copies:
            copy.start()
        for copy in copies:
            copy.wait()

    where = pl.BlockSpec(memory_space=pl.ANY)
    return pl.pallas_call(
        kernel,
        out_shape=[jax.ShapeDtypeStruct((n, width), arrays[0].dtype) for n in rows],
        in_specs=[where] * len(arrays),
        out_specs=[where] * len(rows),
        scratch_shapes=[pltpu.SemaphoreType.DMA((len(plan),))],
    )(*arrays)


def own_rows(z, y, back_z, back_y):
    return pl.multiple_of((((z - back_z) % 8) * 4 + (y - back_y) % 4) * 64, 64)


def pack_kernel(recur_in, branch_in, recur_out_t, gate, up, down_t, narrow, wide):
    wide[:, 0:704] = gate[...]
    wide[:, 704:1408] = up[...]
    narrow[0:64] = recur_out_t[...]
    narrow[64:128] = recur_in[...]
    narrow[128:192] = branch_in[...]
    for t in range(5):
        narrow[192 + t * 64 : 256 + t * 64] = down_t[:, t * 128 : t * 128 + 128]
    narrow[512:544, 0:64] = down_t[0:32, 640:704]
    narrow[512:544, 64:128] = down_t[32:64, 640:704]


def sigmoid(v):
    return 1.0 / (1.0 + jnp.exp(-v))


def one_minus_exp(v):
    series = jnp.ones_like(v)
    for n in range(9, 1, -1):
        series = 1.0 + v * (1.0 / n) * series
    return jnp.where(v > -0.5, -v * series, 1.0 - jnp.exp(v))


def nt_dot(left, right):
    return lax.dot_general(
        left, right, (((1,), (1,)), ((), ())), preferred_element_type=jnp.float32
    )


def recurrent_kernel(where, *refs):
    toks = refs[0:4]
    others = refs[4]
    gain, conv_taps, recur_gate, input_gate, coefs, out_gains = refs[5:11]
    pieces_in = refs[11:15]
    recur_out = refs[15]
    normed, w_in, gates, padded, a_s, b_s, cum_s = refs[16:]
    x, c, z, y = where[0], where[1], where[2], where[3]
    own = pl.ds(pl.multiple_of((2 * x + c) * 128, 128), 128)
    taps = conv_taps[:, own].astype(jnp.float32)
    coef = coefs[:, own]
    out_gain = out_gains[:, own]
    gates[...] = jnp.zeros(gates.shape, jnp.bfloat16)
    for d in range(2):
        for kind, ref in enumerate((recur_gate, input_gate)):
            for g in range(2):
                first = (2 * d + kind) * 128 + g * BLOCK
                gates[g * BLOCK : (g + 1) * BLOCK, first : first + BLOCK] = ref[
                    d, 2 * (2 * x + c) + g
                ]
    chunks = [(toks[k], 2 * ((x - k) % 4) + c) for k in range(4)]
    chunks += [(others.at[k], 2 * ((x - k) % 4) + 1 - c) for k in range(4)]
    energy = None
    for ref, _ in chunks:
        v = ref[...].astype(jnp.float32)
        e = jnp.sum(v * v, axis=1, keepdims=True)
        energy = e if energy is None else energy + e
    scale = lax.rsqrt(energy / D + EPS)
    for ref, at in chunks:
        cols = pl.ds(pl.multiple_of(at * 256, 256), 256)
        v = ref[...].astype(jnp.float32)
        normed[:, cols] = (v * scale * gain[:, cols]).astype(jnp.bfloat16)
    for back_y, ref in enumerate(pieces_in):
        for back_z in range(8):
            at = pl.ds(own_rows(z, y, back_z, back_y), 64)
            w_in[at, 0:128] = ref[back_z * 192 + 64 : back_z * 192 + 128, :]
            w_in[at, 128:256] = ref[back_z * 192 + 128 : back_z * 192 + 192, :]
    both = jnp.dot(normed[...], w_in[...], preferred_element_type=jnp.float32)
    recur_x = both[:, 0:128].astype(jnp.bfloat16).astype(jnp.float32)
    branch_x = both[:, 128:256].astype(jnp.bfloat16).astype(jnp.float32)
    length = recur_x.shape[0]
    padded[0:8, :] = jnp.zeros((8, 128), jnp.float32)
    padded[length + 8 : length + 16, :] = jnp.zeros((8, 128), jnp.float32)
    padded[8 : length + 8, :] = recur_x
    conv = taps[0:1, :] * padded[6 : length + 6, :]
    for k in range(1, 4):
        conv = conv + taps[k : k + 1, :] * padded[6 + k : length + 6 + k, :]
    weight = gates[...]
    high = conv.astype(jnp.bfloat16)
    rest = conv - high.astype(jnp.float32)
    mid = rest.astype(jnp.bfloat16)
    low = (rest - mid.astype(jnp.float32)).astype(jnp.bfloat16)
    mapped = (
        jnp.dot(low, weight, preferred_element_type=jnp.float32)
        + jnp.dot(mid, weight, preferred_element_type=jnp.float32)
    ) + jnp.dot(high, weight, preferred_element_type=jnp.float32)
    count = length // SEG
    for d in range(2):
        rate = sigmoid(mapped[:, d * 256 : d * 256 + 128])
        inlet = sigmoid(mapped[:, d * 256 + 128 : d * 256 + 256])
        log_decay = rate * coef[d : d + 1, :]
        inflow = conv * inlet * jnp.sqrt(one_minus_exp(2.0 * log_decay))
        decay = jnp.exp(log_decay)
        for s in range(count):
            a_s[d, s * PAD_SEG : s * PAD_SEG + SEG, :] = decay[s * SEG : s * SEG + SEG]
            b_s[d, s * PAD_SEG : s * PAD_SEG + SEG, :] = inflow[s * SEG : s * SEG + SEG]
    state = [jnp.zeros((count, 128), jnp.float32) for _ in range(2)]
    through = [jnp.ones((count, 128), jnp.float32) for _ in range(2)]
    for j in range(SEG):
        for d in range(2):
            at = pl.ds(j if d == 0 else SEG - 1 - j, count, stride=PAD_SEG)
            a = a_s[d, at, :]
            state[d] = a * state[d] + b_s[d, at, :]
            through[d] = a * through[d]
            b_s[d, at, :] = state[d]
            cum_s[d, at, :] = through[d]
    carries = [[None] * count for _ in range(2)]
    for d in range(2):
        order = list(range(count)) if d == 0 else list(range(count - 1, -1, -1))
        carry = jnp.zeros((1, 128), jnp.float32)
        for s in order:
            carries[d][s] = carry
            carry = through[d][s : s + 1] * carry + state[d][s : s + 1]
    summed = []
    for s in range(count):
        at = slice(s * PAD_SEG, s * PAD_SEG + SEG)
        summed.append(
            (b_s[0, at, :] + cum_s[0, at, :] * carries[0][s])
            + (b_s[1, at, :] + cum_s[1, at, :] * carries[1][s])
        )
    mixed = jnp.concatenate(summed, axis=0) * jax.nn.gelu(branch_x, approximate=True)
    recur_out[...] = (mixed * out_gain).astype(jnp.bfloat16)


def middle_kernel(where, *refs):
    toks = refs[0:4]
    tok_others = refs[4]
    recur = refs[5:9]
    recur_others = refs[9]
    weights = refs[10:14]
    weight_others = refs[14]
    post, gain = refs[15:17]
    normed, mid_own = refs[17:19]
    left, right, mid = refs[19:]
    x, c, z, y = where[0], where[1], where[2], where[3]
    for k in range(4):
        left[:, k * 128 : k * 128 + 128] = recur[k][...]
        left[:, 512 + k * 128 : 640 + k * 128] = recur_others[k]
        for back_y in range(4):
            for back_z in range(8):
                at = pl.ds(own_rows(z, y, back_z, back_y), 64)
                come = slice((back_y * 8 + back_z) * 64, (back_y * 8 + back_z) * 64 + 64)
                right[at, k * 128 : k * 128 + 128] = weights[k][come, :]
                right[at, 512 + k * 128 : 640 + k * 128] = weight_others[k, come, :]
    total = nt_dot(left[...], right[...])
    scale = lax.rsqrt(jnp.sum(total * total, axis=1, keepdims=True) / D + EPS)
    mid[...] = total * scale * post[...]
    chunks = [(toks[k], 2 * ((x - k) % 4) + c) for k in range(4)]
    chunks += [(tok_others.at[k], 2 * ((x - k) % 4) + 1 - c) for k in range(4)]
    energy = None
    for tok, at in chunks:
        cols = pl.ds(pl.multiple_of(at * 256, 256), 256)
        v = (tok[...].astype(jnp.float32) + mid[:, cols]).astype(jnp.bfloat16)
        if tok is toks[0]:
            mid_own[...] = v
        v = v.astype(jnp.float32)
        mid[:, cols] = v
        e = jnp.sum(v * v, axis=1, keepdims=True)
        energy = e if energy is None else energy + e
    scale = lax.rsqrt(energy / D + EPS)
    for at in range(8):
        cols = slice(at * 256, at * 256 + 256)
        normed[:, cols] = (mid[:, cols] * scale * gain[:, cols]).astype(jnp.bfloat16)


def forward_kernel(where, normed, *refs):
    blocks = refs[0:8]
    pieces_in = refs[8:12]
    keep, send = refs[12:14]
    w_in, w_out = refs[14:]
    c, z, y = where[1], where[2], where[3]
    for back_z, ref in enumerate(blocks):
        for back_y in range(4):
            at = pl.ds(own_rows(z, y, back_z, back_y), 64)
            w_in[at, :] = ref[back_y * 64 : back_y * 64 + 64, :]
    for back_z in range(8):
        at_z = (z - back_z) % 8
        core, at_x = at_z % 2, at_z // 2
        for back_y, ref in enumerate(pieces_in):
            first = pl.multiple_of(at_x * 256 + ((y - back_y) % 4) * 64, 64)
            come = back_z * 352
            for t in range(5):
                w_out[core, pl.ds(first, 64), t * 128 : t * 128 + 128] = ref[
                    come + t * 64 : come + t * 64 + 64, :
                ]
            last = ref[come + 320 : come + 352, :]
            w_out[core, pl.ds(first, 32), 640:704] = last[:, 0:64]
            w_out[core, pl.ds(first + 32, 32), 640:704] = last[:, 64:128]
    both = jnp.dot(normed[...], w_in[...], preferred_element_type=jnp.float32)
    width = both.shape[1] // 2
    gate = both[:, :width]
    hidden = (gate * sigmoid(gate) * both[:, width:]).astype(jnp.bfloat16)
    for to in range(4):
        rows = slice(to * 256, to * 256 + 256)
        send[to] = nt_dot(hidden, w_out[1 - c, rows, :]).astype(jnp.bfloat16)
        keep[to] = nt_dot(hidden, w_out[c, rows, :]).astype(jnp.bfloat16)


VMEM = pl.BlockSpec(memory_space=pltpu.MemorySpace.VMEM)
SMEM = pl.BlockSpec(memory_space=pltpu.MemorySpace.SMEM)


def on_device(
    tokens,
    mixer_gain,
    recur_in,
    branch_in,
    conv_taps,
    recur_gate,
    input_gate,
    decay_param,
    recur_gain,
    recur_out,
    mixer_post,
    channel_gain,
    hidden_gate,
    hidden_up,
    hidden_down,
    channel_post,
):
    x, c = lax.axis_index("x"), lax.axis_index("c")
    rank_tp = 2 * x + c
    length, feature_width = tokens.shape
    channels = recur_in.shape[1]
    rows = recur_in.shape[0]
    width = hidden_gate.shape[1]
    where = jnp.stack([x, c, lax.axis_index("z"), lax.axis_index("y")]).astype(jnp.int32)

    narrow, wide = pl.pallas_call(
        pack_kernel,
        out_shape=(
            jax.ShapeDtypeStruct((3 * rows + width // 2, 128), jnp.bfloat16),
            jax.ShapeDtypeStruct((rows, 2 * width), jnp.bfloat16),
        ),
        in_specs=[VMEM] * 6,
        out_specs=(VMEM, VMEM),
        name="pack",
    )(recur_in, branch_in, recur_out.T, hidden_gate, hidden_up, hidden_down.T)
    narrow_z = along_z(narrow)
    recur_z, down_z = copied(
        [(k, 0, 0, k * 3 * rows, 3 * rows) for k in range(8)]
        + [(k, 3 * rows, 1, k * width // 2, width // 2) for k in range(8)],
        narrow_z,
        (24 * rows, 4 * width),
    )
    wide_y = from_all_y(wide)
    (wide_joined,) = copied(
        [(k, 0, 0, k * rows, rows) for k in range(4)], wide_y, (4 * rows,)
    )
    toks = from_all_x(tokens)
    hidden_blocks = along_z(wide_joined)
    tok_others = swap_cores(jnp.stack(toks))
    recur_pieces = from_all_y(recur_z)
    down_y = from_all_y(down_z)
    (weights,) = copied(
        [
            (ky, kz * 3 * rows, 0, (ky * 8 + kz) * rows, rows)
            for ky in range(4)
            for kz in range(8)
        ],
        recur_pieces,
        (D,),
    )
    weights = from_all_x(weights)
    weight_others = swap_cores(jnp.stack(weights))
    coef = -SHRINK * jax.nn.softplus(-decay_param)

    seg_rows = (length // SEG) * PAD_SEG
    recur_y = pl.pallas_call(
        recurrent_kernel,
        out_shape=jax.ShapeDtypeStruct((length, channels), jnp.bfloat16),
        in_specs=[SMEM] + [VMEM] * 15,
        out_specs=VMEM,
        scratch_shapes=[
            pltpu.VMEM((length, D), jnp.bfloat16),
            pltpu.VMEM((D, 256), jnp.bfloat16),
            pltpu.VMEM((channels, 4 * channels), jnp.bfloat16),
            pltpu.VMEM((length + 16, channels), jnp.float32),
            pltpu.VMEM((2, seg_rows, channels), jnp.float32),
            pltpu.VMEM((2, seg_rows, channels), jnp.float32),
            pltpu.VMEM((2, seg_rows, channels), jnp.float32),
        ],
        name="recurrent",
    )(
        where,
        *toks,
        tok_others,
        mixer_gain[None],
        conv_taps,
        recur_gate,
        input_gate,
        coef,
        recur_gain[None],
        *recur_pieces,
    )
    recur = from_all_x(recur_y)
    recur_others = swap_cores(jnp.stack(recur))
    normed, mid_own = pl.pallas_call(
        middle_kernel,
        out_shape=(
            jax.ShapeDtypeStruct((length, D), jnp.bfloat16),
            jax.ShapeDtypeStruct((length, feature_width), jnp.bfloat16),
        ),
        in_specs=[SMEM] + [VMEM] * 17,
        out_specs=(VMEM, VMEM),
        scratch_shapes=[
            pltpu.VMEM((length, 8 * channels), jnp.bfloat16),
            pltpu.VMEM((D, 8 * channels), jnp.bfloat16),
            pltpu.VMEM((length, D), jnp.float32),
        ],
        name="middle",
    )(
        where,
        *toks,
        tok_others,
        *recur,
        recur_others,
        *weights,
        weight_others,
        mixer_post[None],
        channel_gain[None],
    )
    keep, send = pl.pallas_call(
        forward_kernel,
        out_shape=(jax.ShapeDtypeStruct((4, length, 256), jnp.bfloat16),) * 2,
        in_specs=[SMEM] + [VMEM] * 13,
        out_specs=(VMEM, VMEM),
        scratch_shapes=[
            pltpu.VMEM((D, 2 * width), jnp.bfloat16),
            pltpu.VMEM((2, D // 2, width), jnp.bfloat16),
        ],
        name="forward",
    )(where, normed, *hidden_blocks, *down_y)
    came = swap_cores(send)

    def pair(to):
        one = lax.dynamic_index_in_dim(keep, to, 0, False).astype(jnp.float32)
        two = lax.dynamic_index_in_dim(came, to, 0, False).astype(jnp.float32)
        return one + two

    hidden_own = pair(x)
    for k in (1, 2, 3):
        part = shift(pair((x + k) % 4).astype(jnp.bfloat16), "x", k)
        hidden_own = hidden_own + part.astype(jnp.float32)
    energy = jnp.sum(hidden_own * hidden_own, axis=1)
    everyone = jnp.broadcast_to(energy, (8, length))
    energy = jnp.sum(lax.all_to_all(everyone, TP, 0, 0, tiled=True), axis=0)
    post_own = lax.dynamic_slice_in_dim(channel_post, rank_tp * feature_width, feature_width, 0)
    return (
        mid_own.astype(jnp.float32)
        + hidden_own * lax.rsqrt(energy / D + EPS)[:, None] * post_own
    ).astype(jnp.bfloat16)


def solution(mesh):
    split = Mesh(mesh.devices.reshape(8, 4, 4, 2), ("z", "y", "x", "c"))
    placed = (
        P(FS, TP),
        P(),
        P(FS, TP),
        P(FS, TP),
        P(),
        P(),
        P(),
        P(),
        P(),
        P(TP, FS),
        P(),
        P(),
        P(FS, TP),
        P(FS, TP),
        P(TP, FS),
        P(),
    )

    return jax.shard_map(on_device, mesh=split, in_specs=placed, out_specs=P(FS, TP), check_vma=False)
```

```python
import jax
import jax.numpy as jnp
from jax import lax
from jax.experimental import pallas as pl
from jax.experimental.pallas import tpu as pltpu
from jax.sharding import Mesh
from jax.sharding import PartitionSpec as P

D = 2048
BLOCK = 64
FS = ("z", "y")
TP = ("x", "c")
EPS = 1e-06
SHRINK = 8.0
SEG = 64
PAD_SEG = 72


def shift(array, axis, by):
    n = lax.axis_size(axis)
    return lax.ppermute(array, axis, [(i, (i + by) % n) for i in range(n)])


def swap_cores(array):
    return lax.ppermute(array, "c", [(0, 1), (1, 0)])


def from_all_x(array):
    return [array] + [shift(array, "x", k) for k in (1, 2, 3)]


def from_all_y(array):
    return [array] + [shift(array, "y", k) for k in (1, 2, 3)]


def along_z(block):
    ahead, behind = [block], [block]
    for _ in range(3):
        ahead.append(shift(ahead[-1], "z", 1))
        behind.append(shift(behind[-1], "z", -1))
    passed = jnp.where(lax.axis_index("c") == 0, ahead[3], behind[3])
    n = lax.axis_size("z")
    pairs = [(2 * i, 2 * ((i + 1) % n)) for i in range(n)]
    pairs += [(2 * i + 1, 2 * ((i - 1) % n) + 1) for i in range(n)]
    last = lax.ppermute(passed, ("z", "c"), pairs)
    return ahead + [last] + behind[:0:-1]


def copied(plan, arrays, rows):
    width = arrays[0].shape[1]

    def kernel(*refs):
        for a, first, b, to, n in plan:
            refs[len(arrays) + b][to : to + n, :] = refs[a][first : first + n, :]

    return pl.pallas_call(
        kernel,
        out_shape=[jax.ShapeDtypeStruct((n, width), arrays[0].dtype) for n in rows],
        in_specs=[VMEM] * len(arrays),
        out_specs=[VMEM] * len(rows),
    )(*arrays)


def own_rows(z, y, back_z, back_y):
    return pl.multiple_of((((z - back_z) % 8) * 4 + (y - back_y) % 4) * 64, 64)


def pack_kernel(recur_in, branch_in, recur_out_t, gate, up, down_t, narrow, wide):
    wide[:, 0:704] = gate[...]
    wide[:, 704:1408] = up[...]
    narrow[0:64] = recur_out_t[...]
    narrow[64:128] = recur_in[...]
    narrow[128:192] = branch_in[...]
    for t in range(5):
        narrow[192 + t * 64 : 256 + t * 64] = down_t[:, t * 128 : t * 128 + 128]
    narrow[512:544, 0:64] = down_t[0:32, 640:704]
    narrow[512:544, 64:128] = down_t[32:64, 640:704]


def sigmoid(v):
    return 1.0 / (1.0 + jnp.exp(-v))


def one_minus_exp(v):
    series = jnp.ones_like(v)
    for n in range(9, 1, -1):
        series = 1.0 + v * (1.0 / n) * series
    return jnp.where(v > -0.5, -v * series, 1.0 - jnp.exp(v))


def nt_dot(left, right):
    return lax.dot_general(
        left, right, (((1,), (1,)), ((), ())), preferred_element_type=jnp.float32
    )


def recurrent_kernel(where, *refs):
    toks = refs[0:4]
    others = refs[4]
    gain, conv_taps, recur_gate, input_gate, coefs, out_gains = refs[5:11]
    pieces_in = refs[11:15]
    recur_out = refs[15]
    normed, w_in, gates, padded, a_s, b_s, cum_s = refs[16:]
    x, c, z, y = where[0], where[1], where[2], where[3]
    own = pl.ds(pl.multiple_of((2 * x + c) * 128, 128), 128)
    taps = conv_taps[:, own].astype(jnp.float32)
    coef = coefs[:, own]
    out_gain = out_gains[:, own]
    gates[...] = jnp.zeros(gates.shape, jnp.bfloat16)
    for d in range(2):
        for kind, ref in enumerate((recur_gate, input_gate)):
            for g in range(2):
                first = (2 * d + kind) * 128 + g * BLOCK
                gates[g * BLOCK : (g + 1) * BLOCK, first : first + BLOCK] = ref[
                    d, 2 * (2 * x + c) + g
                ]
    chunks = [(toks[k], 2 * ((x - k) % 4) + c) for k in range(4)]
    chunks += [(others.at[k], 2 * ((x - k) % 4) + 1 - c) for k in range(4)]
    energy = None
    for ref, _ in chunks:
        v = ref[...].astype(jnp.float32)
        e = jnp.sum(v * v, axis=1, keepdims=True)
        energy = e if energy is None else energy + e
    scale = lax.rsqrt(energy / D + EPS)
    for ref, at in chunks:
        cols = pl.ds(pl.multiple_of(at * 256, 256), 256)
        v = ref[...].astype(jnp.float32)
        normed[:, cols] = (v * scale * gain[:, cols]).astype(jnp.bfloat16)
    for back_y, ref in enumerate(pieces_in):
        for back_z in range(8):
            at = pl.ds(own_rows(z, y, back_z, back_y), 64)
            w_in[at, 0:128] = ref[back_z * 192 + 64 : back_z * 192 + 128, :]
            w_in[at, 128:256] = ref[back_z * 192 + 128 : back_z * 192 + 192, :]
    both = jnp.dot(normed[...], w_in[...], preferred_element_type=jnp.float32)
    recur_x = both[:, 0:128].astype(jnp.bfloat16).astype(jnp.float32)
    branch_x = both[:, 128:256].astype(jnp.bfloat16).astype(jnp.float32)
    length = recur_x.shape[0]
    padded[0:8, :] = jnp.zeros((8, 128), jnp.float32)
    padded[length + 8 : length + 16, :] = jnp.zeros((8, 128), jnp.float32)
    padded[8 : length + 8, :] = recur_x
    conv = taps[0:1, :] * padded[6 : length + 6, :]
    for k in range(1, 4):
        conv = conv + taps[k : k + 1, :] * padded[6 + k : length + 6 + k, :]
    weight = gates[...]
    high = conv.astype(jnp.bfloat16)
    rest = conv - high.astype(jnp.float32)
    mid = rest.astype(jnp.bfloat16)
    low = (rest - mid.astype(jnp.float32)).astype(jnp.bfloat16)
    mapped = (
        jnp.dot(low, weight, preferred_element_type=jnp.float32)
        + jnp.dot(mid, weight, preferred_element_type=jnp.float32)
    ) + jnp.dot(high, weight, preferred_element_type=jnp.float32)
    count = length // SEG
    for d in range(2):
        rate = sigmoid(mapped[:, d * 256 : d * 256 + 128])
        inlet = sigmoid(mapped[:, d * 256 + 128 : d * 256 + 256])
        log_decay = rate * coef[d : d + 1, :]
        inflow = conv * inlet * jnp.sqrt(one_minus_exp(2.0 * log_decay))
        decay = jnp.exp(log_decay)
        for s in range(count):
            a_s[d, s * PAD_SEG : s * PAD_SEG + SEG, :] = decay[s * SEG : s * SEG + SEG]
            b_s[d, s * PAD_SEG : s * PAD_SEG + SEG, :] = inflow[s * SEG : s * SEG + SEG]
    state = [jnp.zeros((count, 128), jnp.float32) for _ in range(2)]
    through = [jnp.ones((count, 128), jnp.float32) for _ in range(2)]
    for j in range(SEG):
        for d in range(2):
            at = pl.ds(j if d == 0 else SEG - 1 - j, count, stride=PAD_SEG)
            a = a_s[d, at, :]
            state[d] = a * state[d] + b_s[d, at, :]
            through[d] = a * through[d]
            b_s[d, at, :] = state[d]
            cum_s[d, at, :] = through[d]
    carries = [[None] * count for _ in range(2)]
    for d in range(2):
        order = list(range(count)) if d == 0 else list(range(count - 1, -1, -1))
        carry = jnp.zeros((1, 128), jnp.float32)
        for s in order:
            carries[d][s] = carry
            carry = through[d][s : s + 1] * carry + state[d][s : s + 1]
    summed = []
    for s in range(count):
        at = slice(s * PAD_SEG, s * PAD_SEG + SEG)
        summed.append(
            (b_s[0, at, :] + cum_s[0, at, :] * carries[0][s])
            + (b_s[1, at, :] + cum_s[1, at, :] * carries[1][s])
        )
    mixed = jnp.concatenate(summed, axis=0) * jax.nn.gelu(branch_x, approximate=True)
    recur_out[...] = (mixed * out_gain).astype(jnp.bfloat16)


def middle_kernel(where, *refs):
    toks = refs[0:4]
    tok_others = refs[4]
    recur = refs[5:9]
    recur_others = refs[9]
    weights = refs[10:14]
    weight_others = refs[14]
    post, gain = refs[15:17]
    normed, mid_own = refs[17:19]
    left, right, mid = refs[19:]
    x, c, z, y = where[0], where[1], where[2], where[3]
    for k in range(4):
        left[:, k * 128 : k * 128 + 128] = recur[k][...]
        left[:, 512 + k * 128 : 640 + k * 128] = recur_others[k]
        for back_y in range(4):
            for back_z in range(8):
                at = pl.ds(own_rows(z, y, back_z, back_y), 64)
                come = slice((back_y * 8 + back_z) * 64, (back_y * 8 + back_z) * 64 + 64)
                right[at, k * 128 : k * 128 + 128] = weights[k][come, :]
                right[at, 512 + k * 128 : 640 + k * 128] = weight_others[k, come, :]
    total = nt_dot(left[...], right[...])
    scale = lax.rsqrt(jnp.sum(total * total, axis=1, keepdims=True) / D + EPS)
    mid[...] = total * scale * post[...]
    chunks = [(toks[k], 2 * ((x - k) % 4) + c) for k in range(4)]
    chunks += [(tok_others.at[k], 2 * ((x - k) % 4) + 1 - c) for k in range(4)]
    energy = None
    for tok, at in chunks:
        cols = pl.ds(pl.multiple_of(at * 256, 256), 256)
        v = (tok[...].astype(jnp.float32) + mid[:, cols]).astype(jnp.bfloat16)
        if tok is toks[0]:
            mid_own[...] = v
        v = v.astype(jnp.float32)
        mid[:, cols] = v
        e = jnp.sum(v * v, axis=1, keepdims=True)
        energy = e if energy is None else energy + e
    scale = lax.rsqrt(energy / D + EPS)
    for at in range(8):
        cols = slice(at * 256, at * 256 + 256)
        normed[:, cols] = (mid[:, cols] * scale * gain[:, cols]).astype(jnp.bfloat16)


def forward_kernel(where, normed, *refs):
    blocks = refs[0:8]
    pieces_in = refs[8:12]
    keep, send = refs[12:14]
    w_in, w_out = refs[14:]
    c, z, y = where[1], where[2], where[3]
    for back_z, ref in enumerate(blocks):
        for back_y in range(4):
            at = pl.ds(own_rows(z, y, back_z, back_y), 64)
            w_in[at, :] = ref[back_y * 64 : back_y * 64 + 64, :]
    for back_z in range(8):
        at_z = (z - back_z) % 8
        core, at_x = at_z % 2, at_z // 2
        for back_y, ref in enumerate(pieces_in):
            first = pl.multiple_of(at_x * 256 + ((y - back_y) % 4) * 64, 64)
            come = back_z * 352
            for t in range(5):
                w_out[core, pl.ds(first, 64), t * 128 : t * 128 + 128] = ref[
                    come + t * 64 : come + t * 64 + 64, :
                ]
            last = ref[come + 320 : come + 352, :]
            w_out[core, pl.ds(first, 32), 640:704] = last[:, 0:64]
            w_out[core, pl.ds(first + 32, 32), 640:704] = last[:, 64:128]
    both = jnp.dot(normed[...], w_in[...], preferred_element_type=jnp.float32)
    width = both.shape[1] // 2
    gate = both[:, :width]
    hidden = (gate * sigmoid(gate) * both[:, width:]).astype(jnp.bfloat16)
    for to in range(4):
        rows = slice(to * 256, to * 256 + 256)
        send[to] = nt_dot(hidden, w_out[1 - c, rows, :]).astype(jnp.bfloat16)
        keep[to] = nt_dot(hidden, w_out[c, rows, :]).astype(jnp.bfloat16)


VMEM = pl.BlockSpec(memory_space=pltpu.MemorySpace.VMEM)
SMEM = pl.BlockSpec(memory_space=pltpu.MemorySpace.SMEM)


def on_device(
    tokens,
    mixer_gain,
    recur_in,
    branch_in,
    conv_taps,
    recur_gate,
    input_gate,
    decay_param,
    recur_gain,
    recur_out,
    mixer_post,
    channel_gain,
    hidden_gate,
    hidden_up,
    hidden_down,
    channel_post,
):
    x, c = lax.axis_index("x"), lax.axis_index("c")
    rank_tp = 2 * x + c
    length, feature_width = tokens.shape
    channels = recur_in.shape[1]
    rows = recur_in.shape[0]
    width = hidden_gate.shape[1]
    where = jnp.stack([x, c, lax.axis_index("z"), lax.axis_index("y")]).astype(jnp.int32)

    narrow, wide = pl.pallas_call(
        pack_kernel,
        out_shape=(
            jax.ShapeDtypeStruct((3 * rows + width // 2, 128), jnp.bfloat16),
            jax.ShapeDtypeStruct((rows, 2 * width), jnp.bfloat16),
        ),
        in_specs=[VMEM] * 6,
        out_specs=(VMEM, VMEM),
        name="pack",
    )(recur_in, branch_in, recur_out.T, hidden_gate, hidden_up, hidden_down.T)
    narrow_z = along_z(narrow)
    recur_z, down_z = copied(
        [(k, 0, 0, k * 3 * rows, 3 * rows) for k in range(8)]
        + [(k, 3 * rows, 1, k * width // 2, width // 2) for k in range(8)],
        narrow_z,
        (24 * rows, 4 * width),
    )
    wide_y = from_all_y(wide)
    (wide_joined,) = copied(
        [(k, 0, 0, k * rows, rows) for k in range(4)], wide_y, (4 * rows,)
    )
    toks = from_all_x(tokens)
    hidden_blocks = along_z(wide_joined)
    tok_others = swap_cores(jnp.stack(toks))
    recur_pieces = from_all_y(recur_z)
    down_y = from_all_y(down_z)
    (weights,) = copied(
        [
            (ky, kz * 3 * rows, 0, (ky * 8 + kz) * rows, rows)
            for ky in range(4)
            for kz in range(8)
        ],
        recur_pieces,
        (D,),
    )
    weights = from_all_x(weights)
    weight_others = swap_cores(jnp.stack(weights))
    coef = -SHRINK * jax.nn.softplus(-decay_param)

    seg_rows = (length // SEG) * PAD_SEG
    recur_y = pl.pallas_call(
        recurrent_kernel,
        out_shape=jax.ShapeDtypeStruct((length, channels), jnp.bfloat16),
        in_specs=[SMEM] + [VMEM] * 15,
        out_specs=VMEM,
        scratch_shapes=[
            pltpu.VMEM((length, D), jnp.bfloat16),
            pltpu.VMEM((D, 256), jnp.bfloat16),
            pltpu.VMEM((channels, 4 * channels), jnp.bfloat16),
            pltpu.VMEM((length + 16, channels), jnp.float32),
            pltpu.VMEM((2, seg_rows, channels), jnp.float32),
            pltpu.VMEM((2, seg_rows, channels), jnp.float32),
            pltpu.VMEM((2, seg_rows, channels), jnp.float32),
        ],
        name="recurrent",
    )(
        where,
        *toks,
        tok_others,
        mixer_gain[None],
        conv_taps,
        recur_gate,
        input_gate,
        coef,
        recur_gain[None],
        *recur_pieces,
    )
    recur = from_all_x(recur_y)
    recur_others = swap_cores(jnp.stack(recur))
    normed, mid_own = pl.pallas_call(
        middle_kernel,
        out_shape=(
            jax.ShapeDtypeStruct((length, D), jnp.bfloat16),
            jax.ShapeDtypeStruct((length, feature_width), jnp.bfloat16),
        ),
        in_specs=[SMEM] + [VMEM] * 17,
        out_specs=(VMEM, VMEM),
        scratch_shapes=[
            pltpu.VMEM((length, 8 * channels), jnp.bfloat16),
            pltpu.VMEM((D, 8 * channels), jnp.bfloat16),
            pltpu.VMEM((length, D), jnp.float32),
        ],
        name="middle",
    )(
        where,
        *toks,
        tok_others,
        *recur,
        recur_others,
        *weights,
        weight_others,
        mixer_post[None],
        channel_gain[None],
    )
    keep, send = pl.pallas_call(
        forward_kernel,
        out_shape=(jax.ShapeDtypeStruct((4, length, 256), jnp.bfloat16),) * 2,
        in_specs=[SMEM] + [VMEM] * 13,
        out_specs=(VMEM, VMEM),
        scratch_shapes=[
            pltpu.VMEM((D, 2 * width), jnp.bfloat16),
            pltpu.VMEM((2, D // 2, width), jnp.bfloat16),
        ],
        name="forward",
    )(where, normed, *hidden_blocks, *down_y)
    came = swap_cores(send)

    def pair(to):
        one = lax.dynamic_index_in_dim(keep, to, 0, False).astype(jnp.float32)
        two = lax.dynamic_index_in_dim(came, to, 0, False).astype(jnp.float32)
        return one + two

    hidden_own = pair(x)
    for k in (1, 2, 3):
        part = shift(pair((x + k) % 4).astype(jnp.bfloat16), "x", k)
        hidden_own = hidden_own + part.astype(jnp.float32)
    energy = jnp.sum(hidden_own * hidden_own, axis=1)
    everyone = jnp.broadcast_to(energy, (8, length))
    energy = jnp.sum(lax.all_to_all(everyone, TP, 0, 0, tiled=True), axis=0)
    post_own = lax.dynamic_slice_in_dim(channel_post, rank_tp * feature_width, feature_width, 0)
    return (
        mid_own.astype(jnp.float32)
        + hidden_own * lax.rsqrt(energy / D + EPS)[:, None] * post_own
    ).astype(jnp.bfloat16)


def solution(mesh):
    split = Mesh(mesh.devices.reshape(8, 4, 4, 2), ("z", "y", "x", "c"))
    placed = (
        P(FS, TP),
        P(),
        P(FS, TP),
        P(FS, TP),
        P(),
        P(),
        P(),
        P(),
        P(),
        P(TP, FS),
        P(),
        P(),
        P(FS, TP),
        P(FS, TP),
        P(TP, FS),
        P(),
    )

    return jax.shard_map(on_device, mesh=split, in_specs=placed, out_specs=P(FS, TP), check_vma=False)
```

```python
import jax
import jax.numpy as jnp
from jax import lax
from jax.experimental import pallas as pl
from jax.experimental.pallas import tpu as pltpu
from jax.sharding import Mesh
from jax.sharding import PartitionSpec as P

D = 2048
BLOCK = 64
FS = ("z", "y")
TP = ("x", "c")
EPS = 1e-06
SHRINK = 8.0
SEG = 64
PAD_SEG = 72


def shift(array, axis, by):
    n = lax.axis_size(axis)
    return lax.ppermute(array, axis, [(i, (i + by) % n) for i in range(n)])


def swap_cores(array):
    return lax.ppermute(array, "c", [(0, 1), (1, 0)])


def from_all_x(array):
    return [array] + [shift(array, "x", k) for k in (1, 2, 3)]


def from_all_y(array):
    return [array] + [shift(array, "y", k) for k in (1, 2, 3)]


def along_z(block, halves):
    half = block.shape[0] // 2
    ahead, behind = [block], [block]
    for _ in range(3):
        ahead.append(shift(ahead[-1], "z", 1))
        behind.append(shift(behind[-1], "z", -1))
    if halves:
        last = [shift(ahead[3][:half], "z", 1), shift(behind[3][half:], "z", -1)]
    else:
        passed = jnp.where(lax.axis_index("c") == 0, ahead[3], behind[3])
        n = lax.axis_size("z")
        pairs = [(2 * i, 2 * ((i + 1) % n)) for i in range(n)]
        pairs += [(2 * i + 1, 2 * ((i - 1) % n) + 1) for i in range(n)]
        last = [lax.ppermute(passed, ("z", "c"), pairs)]
    return ahead + last + behind[:0:-1]


def copied(plan, arrays, rows):
    width = arrays[0].shape[1]

    def kernel(*refs):
        for a, first, b, to, n in plan:
            refs[len(arrays) + b][to : to + n, :] = refs[a][first : first + n, :]

    return pl.pallas_call(
        kernel,
        out_shape=[jax.ShapeDtypeStruct((n, width), arrays[0].dtype) for n in rows],
        in_specs=[VMEM] * len(arrays),
        out_specs=[VMEM] * len(rows),
    )(*arrays)


def own_rows(z, y, back_z, back_y):
    return pl.multiple_of((((z - back_z) % 8) * 4 + (y - back_y) % 4) * 64, 64)


def pack_kernel(recur_in, branch_in, recur_out_t, gate, up, down_t, narrow, wide):
    wide[:, 0:704] = gate[...]
    wide[:, 704:1408] = up[...]
    narrow[0:64] = recur_out_t[...]
    narrow[64:128] = recur_in[...]
    narrow[128:192] = branch_in[...]
    for t in range(5):
        narrow[192 + t * 64 : 256 + t * 64] = down_t[:, t * 128 : t * 128 + 128]
    narrow[512:544, 0:64] = down_t[0:32, 640:704]
    narrow[512:544, 64:128] = down_t[32:64, 640:704]


def sigmoid(v):
    return 1.0 / (1.0 + jnp.exp(-v))


def one_minus_exp(v):
    series = jnp.ones_like(v)
    for n in range(9, 1, -1):
        series = 1.0 + v * (1.0 / n) * series
    return jnp.where(v > -0.5, -v * series, 1.0 - jnp.exp(v))


def nt_dot(left, right):
    return lax.dot_general(
        left, right, (((1,), (1,)), ((), ())), preferred_element_type=jnp.float32
    )


def norm_kernel(where, *refs):
    toks = refs[0:4]
    others = refs[4]
    gain, normed = refs[5:]
    x, c = where[0], where[1]
    chunks = [(toks[k], 2 * ((x - k) % 4) + c) for k in range(4)]
    chunks += [(others.at[k], 2 * ((x - k) % 4) + 1 - c) for k in range(4)]
    energy = None
    for ref, _ in chunks:
        v = ref[...].astype(jnp.float32)
        e = jnp.sum(v * v, axis=1, keepdims=True)
        energy = e if energy is None else energy + e
    scale = lax.rsqrt(energy / D + EPS)
    for ref, at in chunks:
        cols = pl.ds(pl.multiple_of(at * 256, 256), 256)
        v = ref[...].astype(jnp.float32)
        normed[:, cols] = (v * scale * gain[:, cols]).astype(jnp.bfloat16)


def recurrent_kernel(where, *refs):
    normed, conv_taps, recur_gate, input_gate, coefs, out_gains = refs[0:6]
    pieces_in = refs[6:10]
    recur_out = refs[10]
    w_in, gates, padded, a_s, b_s, cum_s = refs[11:]
    x, c, z, y = where[0], where[1], where[2], where[3]
    own = pl.ds(pl.multiple_of((2 * x + c) * 128, 128), 128)
    taps = conv_taps[:, own].astype(jnp.float32)
    coef = coefs[:, own]
    out_gain = out_gains[:, own]
    gates[...] = jnp.zeros(gates.shape, jnp.bfloat16)
    for d in range(2):
        for kind, ref in enumerate((recur_gate, input_gate)):
            for g in range(2):
                first = (2 * d + kind) * 128 + g * BLOCK
                gates[g * BLOCK : (g + 1) * BLOCK, first : first + BLOCK] = ref[
                    d, 2 * (2 * x + c) + g
                ]
    for back_y, ref in enumerate(pieces_in):
        for back_z in range(8):
            at = pl.ds(own_rows(z, y, back_z, back_y), 64)
            w_in[at, 0:128] = ref[back_z * 192 + 64 : back_z * 192 + 128, :]
            w_in[at, 128:256] = ref[back_z * 192 + 128 : back_z * 192 + 192, :]
    both = jnp.dot(normed[...], w_in[...], preferred_element_type=jnp.float32)
    recur_x = both[:, 0:128].astype(jnp.bfloat16).astype(jnp.float32)
    branch_x = both[:, 128:256].astype(jnp.bfloat16).astype(jnp.float32)
    length = recur_x.shape[0]
    padded[0:8, :] = jnp.zeros((8, 128), jnp.float32)
    padded[length + 8 : length + 16, :] = jnp.zeros((8, 128), jnp.float32)
    padded[8 : length + 8, :] = recur_x
    conv = taps[0:1, :] * padded[6 : length + 6, :]
    for k in range(1, 4):
        conv = conv + taps[k : k + 1, :] * padded[6 + k : length + 6 + k, :]
    weight = gates[...]
    high = conv.astype(jnp.bfloat16)
    rest = conv - high.astype(jnp.float32)
    mid = rest.astype(jnp.bfloat16)
    low = (rest - mid.astype(jnp.float32)).astype(jnp.bfloat16)
    mapped = (
        jnp.dot(low, weight, preferred_element_type=jnp.float32)
        + jnp.dot(mid, weight, preferred_element_type=jnp.float32)
    ) + jnp.dot(high, weight, preferred_element_type=jnp.float32)
    count = length // SEG
    for d in range(2):
        rate = sigmoid(mapped[:, d * 256 : d * 256 + 128])
        inlet = sigmoid(mapped[:, d * 256 + 128 : d * 256 + 256])
        log_decay = rate * coef[d : d + 1, :]
        inflow = conv * inlet * jnp.sqrt(one_minus_exp(2.0 * log_decay))
        decay = jnp.exp(log_decay)
        for s in range(count):
            a_s[d, s * PAD_SEG : s * PAD_SEG + SEG, :] = decay[s * SEG : s * SEG + SEG]
            b_s[d, s * PAD_SEG : s * PAD_SEG + SEG, :] = inflow[s * SEG : s * SEG + SEG]
    state = [jnp.zeros((count, 128), jnp.float32) for _ in range(2)]
    through = [jnp.ones((count, 128), jnp.float32) for _ in range(2)]
    for j in range(SEG):
        for d in range(2):
            at = pl.ds(j if d == 0 else SEG - 1 - j, count, stride=PAD_SEG)
            a = a_s[d, at, :]
            state[d] = a * state[d] + b_s[d, at, :]
            through[d] = a * through[d]
            b_s[d, at, :] = state[d]
            cum_s[d, at, :] = through[d]
    carries = [[None] * count for _ in range(2)]
    for d in range(2):
        order = list(range(count)) if d == 0 else list(range(count - 1, -1, -1))
        carry = jnp.zeros((1, 128), jnp.float32)
        for s in order:
            carries[d][s] = carry
            carry = through[d][s : s + 1] * carry + state[d][s : s + 1]
    summed = []
    for s in range(count):
        at = slice(s * PAD_SEG, s * PAD_SEG + SEG)
        summed.append(
            (b_s[0, at, :] + cum_s[0, at, :] * carries[0][s])
            + (b_s[1, at, :] + cum_s[1, at, :] * carries[1][s])
        )
    mixed = jnp.concatenate(summed, axis=0) * jax.nn.gelu(branch_x, approximate=True)
    recur_out[...] = (mixed * out_gain).astype(jnp.bfloat16)


def middle_kernel(where, *refs):
    toks = refs[0:4]
    tok_others = refs[4]
    recur = refs[5:9]
    recur_others = refs[9]
    weights = refs[10:14]
    weight_others = refs[14]
    post, gain = refs[15:17]
    normed, mid_own = refs[17:19]
    left, right, mid = refs[19:]
    x, c, z, y = where[0], where[1], where[2], where[3]
    for k in range(4):
        left[:, k * 128 : k * 128 + 128] = recur[k][...]
        left[:, 512 + k * 128 : 640 + k * 128] = recur_others[k]
        for back_y in range(4):
            for back_z in range(8):
                at = pl.ds(own_rows(z, y, back_z, back_y), 64)
                come = slice((back_y * 8 + back_z) * 64, (back_y * 8 + back_z) * 64 + 64)
                right[at, k * 128 : k * 128 + 128] = weights[k][come, :]
                right[at, 512 + k * 128 : 640 + k * 128] = weight_others[k, come, :]
    total = nt_dot(left[...], right[...])
    scale = lax.rsqrt(jnp.sum(total * total, axis=1, keepdims=True) / D + EPS)
    mid[...] = total * scale * post[...]
    chunks = [(toks[k], 2 * ((x - k) % 4) + c) for k in range(4)]
    chunks += [(tok_others.at[k], 2 * ((x - k) % 4) + 1 - c) for k in range(4)]
    energy = None
    for tok, at in chunks:
        cols = pl.ds(pl.multiple_of(at * 256, 256), 256)
        v = (tok[...].astype(jnp.float32) + mid[:, cols]).astype(jnp.bfloat16)
        if tok is toks[0]:
            mid_own[...] = v
        v = v.astype(jnp.float32)
        mid[:, cols] = v
        e = jnp.sum(v * v, axis=1, keepdims=True)
        energy = e if energy is None else energy + e
    scale = lax.rsqrt(energy / D + EPS)
    for at in range(8):
        cols = slice(at * 256, at * 256 + 256)
        normed[:, cols] = (mid[:, cols] * scale * gain[:, cols]).astype(jnp.bfloat16)


def forward_kernel(where, normed, *refs):
    blocks = refs[0:9]
    hidden, w_in = refs[9:]
    z, y = where[2], where[3]
    for n, ref in enumerate(blocks):
        back_z = (0, 1, 2, 3, 4, 4, 5, 6, 7)[n]
        for part in range(ref.shape[0] // 64):
            at = pl.ds(own_rows(z, y, back_z, part + (2 if n == 5 else 0)), 64)
            w_in[at, :] = ref[part * 64 : part * 64 + 64, :]
    both = jnp.dot(normed[...], w_in[...], preferred_element_type=jnp.float32)
    width = both.shape[1] // 2
    gate = both[:, :width]
    hidden[...] = (gate * sigmoid(gate) * both[:, width:]).astype(jnp.bfloat16)


def down_kernel(where, hidden, *refs):
    pieces_in = refs[0:4]
    keep, send, w_out = refs[4:]
    c, z, y = where[1], where[2], where[3]
    for back_z in range(8):
        at_z = (z - back_z) % 8
        core, at_x = at_z % 2, at_z // 2
        for back_y, ref in enumerate(pieces_in):
            first = pl.multiple_of(at_x * 256 + ((y - back_y) % 4) * 64, 64)
            come = back_z * 352
            for t in range(5):
                w_out[core, pl.ds(first, 64), t * 128 : t * 128 + 128] = ref[
                    come + t * 64 : come + t * 64 + 64, :
                ]
            last = ref[come + 320 : come + 352, :]
            w_out[core, pl.ds(first, 32), 640:704] = last[:, 0:64]
            w_out[core, pl.ds(first + 32, 32), 640:704] = last[:, 64:128]
    for to in range(4):
        rows = slice(to * 256, to * 256 + 256)
        send[to] = nt_dot(hidden[...], w_out[1 - c, rows, :]).astype(jnp.bfloat16)
        keep[to] = nt_dot(hidden[...], w_out[c, rows, :]).astype(jnp.bfloat16)


VMEM = pl.BlockSpec(memory_space=pltpu.MemorySpace.VMEM)
SMEM = pl.BlockSpec(memory_space=pltpu.MemorySpace.SMEM)


def on_device(
    tokens,
    mixer_gain,
    recur_in,
    branch_in,
    conv_taps,
    recur_gate,
    input_gate,
    decay_param,
    recur_gain,
    recur_out,
    mixer_post,
    channel_gain,
    hidden_gate,
    hidden_up,
    hidden_down,
    channel_post,
):
    x, c = lax.axis_index("x"), lax.axis_index("c")
    rank_tp = 2 * x + c
    length, feature_width = tokens.shape
    channels = recur_in.shape[1]
    rows = recur_in.shape[0]
    width = hidden_gate.shape[1]
    where = jnp.stack([x, c, lax.axis_index("z"), lax.axis_index("y")]).astype(jnp.int32)

    narrow, wide = pl.pallas_call(
        pack_kernel,
        out_shape=(
            jax.ShapeDtypeStruct((3 * rows + width // 2, 128), jnp.bfloat16),
            jax.ShapeDtypeStruct((rows, 2 * width), jnp.bfloat16),
        ),
        in_specs=[VMEM] * 6,
        out_specs=(VMEM, VMEM),
        name="pack",
    )(recur_in, branch_in, recur_out.T, hidden_gate, hidden_up, hidden_down.T)
    narrow_z = along_z(narrow, False)
    recur_z, down_z = copied(
        [(k, 0, 0, k * 3 * rows, 3 * rows) for k in range(8)]
        + [(k, 3 * rows, 1, k * width // 2, width // 2) for k in range(8)],
        narrow_z,
        (24 * rows, 4 * width),
    )
    wide_y = from_all_y(wide)
    (wide_joined,) = copied(
        [(k, 0, 0, k * rows, rows) for k in range(4)], wide_y, (4 * rows,)
    )
    toks = from_all_x(tokens)
    hidden_blocks = along_z(wide_joined, True)
    tok_others = swap_cores(jnp.stack(toks))
    recur_pieces = from_all_y(recur_z)
    down_y = from_all_y(down_z)
    (weights,) = copied(
        [
            (ky, kz * 3 * rows, 0, (ky * 8 + kz) * rows, rows)
            for ky in range(4)
            for kz in range(8)
        ],
        recur_pieces,
        (D,),
    )
    weights = from_all_x(weights)
    weight_others = swap_cores(jnp.stack(weights))
    coef = -SHRINK * jax.nn.softplus(-decay_param)

    seg_rows = (length // SEG) * PAD_SEG
    normed_in = pl.pallas_call(
        norm_kernel,
        out_shape=jax.ShapeDtypeStruct((length, D), jnp.bfloat16),
        in_specs=[SMEM] + [VMEM] * 6,
        out_specs=VMEM,
        name="norm",
    )(where, *toks, tok_others, mixer_gain[None])
    recur_y = pl.pallas_call(
        recurrent_kernel,
        out_shape=jax.ShapeDtypeStruct((length, channels), jnp.bfloat16),
        in_specs=[SMEM] + [VMEM] * 10,
        out_specs=VMEM,
        scratch_shapes=[
            pltpu.VMEM((D, 256), jnp.bfloat16),
            pltpu.VMEM((channels, 4 * channels), jnp.bfloat16),
            pltpu.VMEM((length + 16, channels), jnp.float32),
            pltpu.VMEM((2, seg_rows, channels), jnp.float32),
            pltpu.VMEM((2, seg_rows, channels), jnp.float32),
            pltpu.VMEM((2, seg_rows, channels), jnp.float32),
        ],
        name="recurrent",
    )(
        where,
        normed_in,
        conv_taps,
        recur_gate,
        input_gate,
        coef,
        recur_gain[None],
        *recur_pieces,
    )
    recur = from_all_x(recur_y)
    recur_others = swap_cores(jnp.stack(recur))
    normed, mid_own = pl.pallas_call(
        middle_kernel,
        out_shape=(
            jax.ShapeDtypeStruct((length, D), jnp.bfloat16),
            jax.ShapeDtypeStruct((length, feature_width), jnp.bfloat16),
        ),
        in_specs=[SMEM] + [VMEM] * 17,
        out_specs=(VMEM, VMEM),
        scratch_shapes=[
            pltpu.VMEM((length, 8 * channels), jnp.bfloat16),
            pltpu.VMEM((D, 8 * channels), jnp.bfloat16),
            pltpu.VMEM((length, D), jnp.float32),
        ],
        name="middle",
    )(
        where,
        *toks,
        tok_others,
        *recur,
        recur_others,
        *weights,
        weight_others,
        mixer_post[None],
        channel_gain[None],
    )
    hidden = pl.pallas_call(
        forward_kernel,
        out_shape=jax.ShapeDtypeStruct((length, width), jnp.bfloat16),
        in_specs=[SMEM] + [VMEM] * 10,
        out_specs=VMEM,
        scratch_shapes=[pltpu.VMEM((D, 2 * width), jnp.bfloat16)],
        name="forward",
    )(where, normed, *hidden_blocks)
    keep, send = pl.pallas_call(
        down_kernel,
        out_shape=(jax.ShapeDtypeStruct((4, length, 256), jnp.bfloat16),) * 2,
        in_specs=[SMEM] + [VMEM] * 5,
        out_specs=(VMEM, VMEM),
        scratch_shapes=[pltpu.VMEM((2, D // 2, width), jnp.bfloat16)],
        name="down",
    )(where, hidden, *down_y)
    came = swap_cores(send)

    def pair(to):
        one = lax.dynamic_index_in_dim(keep, to, 0, False).astype(jnp.float32)
        two = lax.dynamic_index_in_dim(came, to, 0, False).astype(jnp.float32)
        return one + two

    hidden_own = pair(x)
    for k in (1, 2, 3):
        part = shift(pair((x + k) % 4).astype(jnp.bfloat16), "x", k)
        hidden_own = hidden_own + part.astype(jnp.float32)
    energy = jnp.sum(hidden_own * hidden_own, axis=1)
    everyone = jnp.broadcast_to(energy, (8, length))
    energy = jnp.sum(lax.all_to_all(everyone, TP, 0, 0, tiled=True), axis=0)
    post_own = lax.dynamic_slice_in_dim(channel_post, rank_tp * feature_width, feature_width, 0)
    return (
        mid_own.astype(jnp.float32)
        + hidden_own * lax.rsqrt(energy / D + EPS)[:, None] * post_own
    ).astype(jnp.bfloat16)


def solution(mesh):
    split = Mesh(mesh.devices.reshape(8, 4, 4, 2), ("z", "y", "x", "c"))
    placed = (
        P(FS, TP),
        P(),
        P(FS, TP),
        P(FS, TP),
        P(),
        P(),
        P(),
        P(),
        P(),
        P(TP, FS),
        P(),
        P(),
        P(FS, TP),
        P(FS, TP),
        P(TP, FS),
        P(),
    )

    return jax.shard_map(on_device, mesh=split, in_specs=placed, out_specs=P(FS, TP), check_vma=False)
```

```python
import jax
import jax.numpy as jnp
from jax import lax
from jax.experimental import pallas as pl
from jax.experimental.pallas import tpu as pltpu
from jax.sharding import Mesh
from jax.sharding import PartitionSpec as P

D = 2048
BLOCK = 64
FS = ("z", "y")
TP = ("x", "c")
EPS = 1e-06
SHRINK = 8.0
SEG = 64
PAD_SEG = 72


def shift(array, axis, by):
    n = lax.axis_size(axis)
    return lax.ppermute(array, axis, [(i, (i + by) % n) for i in range(n)])


def swap_cores(array):
    return lax.ppermute(array, "c", [(0, 1), (1, 0)])


def from_all_x(array):
    return [array] + [shift(array, "x", k) for k in (1, 2, 3)]


def from_all_y(array):
    return [array] + [shift(array, "y", k) for k in (1, 2, 3)]


def along_z(block, halves):
    half = block.shape[0] // 2
    ahead, behind = [block], [block]
    for _ in range(3):
        ahead.append(shift(ahead[-1], "z", 1))
        behind.append(shift(behind[-1], "z", -1))
    if halves:
        last = [shift(ahead[3][:half], "z", 1), shift(behind[3][half:], "z", -1)]
    else:
        passed = jnp.where(lax.axis_index("c") == 0, ahead[3], behind[3])
        n = lax.axis_size("z")
        pairs = [(2 * i, 2 * ((i + 1) % n)) for i in range(n)]
        pairs += [(2 * i + 1, 2 * ((i - 1) % n) + 1) for i in range(n)]
        last = [lax.ppermute(passed, ("z", "c"), pairs)]
    return ahead + last + behind[:0:-1]


def copied(plan, arrays, rows):
    width = arrays[0].shape[1]

    def kernel(*refs):
        for a, first, b, to, n in plan:
            refs[len(arrays) + b][to : to + n, :] = refs[a][first : first + n, :]

    return pl.pallas_call(
        kernel,
        out_shape=[jax.ShapeDtypeStruct((n, width), arrays[0].dtype) for n in rows],
        in_specs=[VMEM] * len(arrays),
        out_specs=[VMEM] * len(rows),
    )(*arrays)


def own_rows(z, y, back_z, back_y):
    return pl.multiple_of((((z - back_z) % 8) * 4 + (y - back_y) % 4) * 64, 64)


def pack_kernel(recur_in, branch_in, recur_out_t, gate, up, down_t, narrow, wide):
    wide[:, 0:704] = gate[...]
    wide[:, 704:1408] = up[...]
    narrow[0:64] = recur_out_t[...]
    narrow[64:128] = recur_in[...]
    narrow[128:192] = branch_in[...]
    for t in range(5):
        narrow[192 + t * 64 : 256 + t * 64] = down_t[:, t * 128 : t * 128 + 128]
    narrow[512:544, 0:64] = down_t[0:32, 640:704]
    narrow[512:544, 64:128] = down_t[32:64, 640:704]


def join_kernel(where, *refs):
    y = where[3]
    for k in range(4):
        refs[4][pl.ds(pl.multiple_of(((y - k) % 4) * 64, 64), 64), :] = refs[k][...]


def sigmoid(v):
    return 1.0 / (1.0 + jnp.exp(-v))


def one_minus_exp(v):
    series = jnp.ones_like(v)
    for n in range(9, 1, -1):
        series = 1.0 + v * (1.0 / n) * series
    return jnp.where(v > -0.5, -v * series, 1.0 - jnp.exp(v))


def nt_dot(left, right):
    return lax.dot_general(
        left, right, (((1,), (1,)), ((), ())), preferred_element_type=jnp.float32
    )


def recurrent_kernel(where, *refs):
    toks = refs[0:4]
    others = refs[4]
    gain, conv_taps, recur_gate, input_gate, coefs, out_gains = refs[5:11]
    pieces_in = refs[11:15]
    recur_out = refs[15]
    normed, w_in, gates, padded, a_s, b_s, cum_s = refs[16:]
    x, c, z, y = where[0], where[1], where[2], where[3]
    own = pl.ds(pl.multiple_of((2 * x + c) * 128, 128), 128)
    taps = conv_taps[:, own].astype(jnp.float32)
    coef = coefs[:, own]
    out_gain = out_gains[:, own]
    gates[...] = jnp.zeros(gates.shape, jnp.bfloat16)
    for d in range(2):
        for kind, ref in enumerate((recur_gate, input_gate)):
            for g in range(2):
                first = (2 * d + kind) * 128 + g * BLOCK
                gates[g * BLOCK : (g + 1) * BLOCK, first : first + BLOCK] = ref[
                    d, 2 * (2 * x + c) + g
                ]
    chunks = [(toks[k], 2 * ((x - k) % 4) + c) for k in range(4)]
    chunks += [(others.at[k], 2 * ((x - k) % 4) + 1 - c) for k in range(4)]
    energy = None
    for ref, _ in chunks:
        v = ref[...].astype(jnp.float32)
        e = jnp.sum(v * v, axis=1, keepdims=True)
        energy = e if energy is None else energy + e
    scale = lax.rsqrt(energy / D + EPS)
    for ref, at in chunks:
        cols = pl.ds(pl.multiple_of(at * 256, 256), 256)
        v = ref[...].astype(jnp.float32)
        normed[:, cols] = (v * scale * gain[:, cols]).astype(jnp.bfloat16)
    for back_y, ref in enumerate(pieces_in):
        for back_z in range(8):
            at = pl.ds(own_rows(z, y, back_z, back_y), 64)
            w_in[at, 0:128] = ref[back_z * 128 : back_z * 128 + 64, :]
            w_in[at, 128:256] = ref[back_z * 128 + 64 : back_z * 128 + 128, :]
    both = jnp.dot(normed[...], w_in[...], preferred_element_type=jnp.float32)
    recur_x = both[:, 0:128].astype(jnp.bfloat16).astype(jnp.float32)
    branch_x = both[:, 128:256].astype(jnp.bfloat16).astype(jnp.float32)
    length = recur_x.shape[0]
    padded[0:8, :] = jnp.zeros((8, 128), jnp.float32)
    padded[length + 8 : length + 16, :] = jnp.zeros((8, 128), jnp.float32)
    padded[8 : length + 8, :] = recur_x
    conv = taps[0:1, :] * padded[6 : length + 6, :]
    for k in range(1, 4):
        conv = conv + taps[k : k + 1, :] * padded[6 + k : length + 6 + k, :]
    weight = gates[...]
    high = conv.astype(jnp.bfloat16)
    rest = conv - high.astype(jnp.float32)
    mid = rest.astype(jnp.bfloat16)
    low = (rest - mid.astype(jnp.float32)).astype(jnp.bfloat16)
    mapped = (
        jnp.dot(low, weight, preferred_element_type=jnp.float32)
        + jnp.dot(mid, weight, preferred_element_type=jnp.float32)
    ) + jnp.dot(high, weight, preferred_element_type=jnp.float32)
    count = length // SEG
    for d in range(2):
        rate = sigmoid(mapped[:, d * 256 : d * 256 + 128])
        inlet = sigmoid(mapped[:, d * 256 + 128 : d * 256 + 256])
        log_decay = rate * coef[d : d + 1, :]
        inflow = conv * inlet * jnp.sqrt(one_minus_exp(2.0 * log_decay))
        decay = jnp.exp(log_decay)
        for s in range(count):
            a_s[d, s * PAD_SEG : s * PAD_SEG + SEG, :] = decay[s * SEG : s * SEG + SEG]
            b_s[d, s * PAD_SEG : s * PAD_SEG + SEG, :] = inflow[s * SEG : s * SEG + SEG]
    state = [jnp.zeros((count, 128), jnp.float32) for _ in range(2)]
    through = [jnp.ones((count, 128), jnp.float32) for _ in range(2)]
    for j in range(SEG):
        for d in range(2):
            at = pl.ds(j if d == 0 else SEG - 1 - j, count, stride=PAD_SEG)
            a = a_s[d, at, :]
            state[d] = a * state[d] + b_s[d, at, :]
            through[d] = a * through[d]
            b_s[d, at, :] = state[d]
            cum_s[d, at, :] = through[d]
    carries = [[None] * count for _ in range(2)]
    for d in range(2):
        order = list(range(count)) if d == 0 else list(range(count - 1, -1, -1))
        carry = jnp.zeros((1, 128), jnp.float32)
        for s in order:
            carries[d][s] = carry
            carry = through[d][s : s + 1] * carry + state[d][s : s + 1]
    summed = []
    for s in range(count):
        at = slice(s * PAD_SEG, s * PAD_SEG + SEG)
        summed.append(
            (b_s[0, at, :] + cum_s[0, at, :] * carries[0][s])
            + (b_s[1, at, :] + cum_s[1, at, :] * carries[1][s])
        )
    mixed = jnp.concatenate(summed, axis=0) * jax.nn.gelu(branch_x, approximate=True)
    recur_out[...] = (mixed * out_gain).astype(jnp.bfloat16)


def middle_kernel(where, *refs):
    toks = refs[0:4]
    tok_others = refs[4]
    recur = refs[5:9]
    recur_others = refs[9]
    weights = refs[10:14]
    weight_others = refs[14]
    post, gain = refs[15:17]
    normed, mid_own = refs[17:19]
    left, right, mid = refs[19:]
    x, c, z, y = where[0], where[1], where[2], where[3]
    for k in range(4):
        left[:, k * 128 : k * 128 + 128] = recur[k][...]
        left[:, 512 + k * 128 : 640 + k * 128] = recur_others[k]
        for back_y in range(4):
            for back_z in range(8):
                at = pl.ds(own_rows(z, y, back_z, back_y), 64)
                come = slice((back_y * 8 + back_z) * 64, (back_y * 8 + back_z) * 64 + 64)
                right[at, k * 128 : k * 128 + 128] = weights[k][come, :]
                right[at, 512 + k * 128 : 640 + k * 128] = weight_others[k, come, :]
    total = nt_dot(left[...], right[...])
    scale = lax.rsqrt(jnp.sum(total * total, axis=1, keepdims=True) / D + EPS)
    mid[...] = total * scale * post[...]
    chunks = [(toks[k], 2 * ((x - k) % 4) + c) for k in range(4)]
    chunks += [(tok_others.at[k], 2 * ((x - k) % 4) + 1 - c) for k in range(4)]
    energy = None
    for tok, at in chunks:
        cols = pl.ds(pl.multiple_of(at * 256, 256), 256)
        v = (tok[...].astype(jnp.float32) + mid[:, cols]).astype(jnp.bfloat16)
        if tok is toks[0]:
            mid_own[...] = v
        v = v.astype(jnp.float32)
        mid[:, cols] = v
        e = jnp.sum(v * v, axis=1, keepdims=True)
        energy = e if energy is None else energy + e
    scale = lax.rsqrt(energy / D + EPS)
    for at in range(8):
        cols = slice(at * 256, at * 256 + 256)
        normed[:, cols] = (mid[:, cols] * scale * gain[:, cols]).astype(jnp.bfloat16)


def forward_kernel(where, normed, *refs):
    blocks = refs[0:9]
    pieces_in = refs[9:13]
    keep, send = refs[13:15]
    w_in, w_out = refs[15:]
    c, z, y = where[1], where[2], where[3]
    for n, ref in enumerate(blocks):
        k = (0, 1, 2, 3, 4, 4, 5, 6, 7)[n]
        start = ((z - k) % 8) * 256 + (128 if n == 5 else 0)
        w_in[pl.ds(pl.multiple_of(start, 128), ref.shape[0]), :] = ref[...]
    for back_z in range(8):
        at_z = (z - back_z) % 8
        core, at_x = at_z % 2, at_z // 2
        for back_y, ref in enumerate(pieces_in):
            first = pl.multiple_of(at_x * 256 + ((y - back_y) % 4) * 64, 64)
            come = back_z * 352
            for t in range(5):
                w_out[core, pl.ds(first, 64), t * 128 : t * 128 + 128] = ref[
                    come + t * 64 : come + t * 64 + 64, :
                ]
            last = ref[come + 320 : come + 352, :]
            w_out[core, pl.ds(first, 32), 640:704] = last[:, 0:64]
            w_out[core, pl.ds(first + 32, 32), 640:704] = last[:, 64:128]
    both = jnp.dot(normed[...], w_in[...], preferred_element_type=jnp.float32)
    width = both.shape[1] // 2
    gate = both[:, :width]
    hidden = (gate * sigmoid(gate) * both[:, width:]).astype(jnp.bfloat16)
    for to in range(4):
        rows = slice(to * 256, to * 256 + 256)
        send[to] = nt_dot(hidden, w_out[1 - c, rows, :]).astype(jnp.bfloat16)
        keep[to] = nt_dot(hidden, w_out[c, rows, :]).astype(jnp.bfloat16)


VMEM = pl.BlockSpec(memory_space=pltpu.MemorySpace.VMEM)
SMEM = pl.BlockSpec(memory_space=pltpu.MemorySpace.SMEM)


def on_device(
    tokens,
    mixer_gain,
    recur_in,
    branch_in,
    conv_taps,
    recur_gate,
    input_gate,
    decay_param,
    recur_gain,
    recur_out,
    mixer_post,
    channel_gain,
    hidden_gate,
    hidden_up,
    hidden_down,
    channel_post,
):
    x, c = lax.axis_index("x"), lax.axis_index("c")
    rank_tp = 2 * x + c
    length, feature_width = tokens.shape
    channels = recur_in.shape[1]
    rows = recur_in.shape[0]
    width = hidden_gate.shape[1]
    where = jnp.stack([x, c, lax.axis_index("z"), lax.axis_index("y")]).astype(jnp.int32)

    narrow, wide = pl.pallas_call(
        pack_kernel,
        out_shape=(
            jax.ShapeDtypeStruct((3 * rows + width // 2, 128), jnp.bfloat16),
            jax.ShapeDtypeStruct((rows, 2 * width), jnp.bfloat16),
        ),
        in_specs=[VMEM] * 6,
        out_specs=(VMEM, VMEM),
        name="pack",
    )(recur_in, branch_in, recur_out.T, hidden_gate, hidden_up, hidden_down.T)
    out_z, in_z, down_z = copied(
        [(k, 0, 0, k * rows, rows) for k in range(8)]
        + [(k, rows, 1, k * 2 * rows, 2 * rows) for k in range(8)]
        + [(k, 3 * rows, 2, k * width // 2, width // 2) for k in range(8)],
        along_z(narrow, False),
        (8 * rows, 16 * rows, 4 * width),
    )
    wide_y = from_all_y(wide)
    hidden_y = pl.pallas_call(
        join_kernel,
        out_shape=jax.ShapeDtypeStruct((4 * rows, 2 * width), jnp.bfloat16),
        in_specs=[SMEM] + [VMEM] * 4,
        out_specs=VMEM,
        name="join",
    )(where, *wide_y)
    toks = from_all_x(tokens)
    hidden_blocks = along_z(hidden_y, True)
    tok_others = swap_cores(jnp.stack(toks))
    out_y = from_all_y(out_z)
    in_y = from_all_y(in_z)
    down_y = from_all_y(down_z)
    (weights,) = copied(
        [(k, 0, 0, k * 8 * rows, 8 * rows) for k in range(4)], out_y, (D,)
    )
    weights = from_all_x(weights)
    weight_others = swap_cores(jnp.stack(weights))
    coef = -SHRINK * jax.nn.softplus(-decay_param)

    seg_rows = (length // SEG) * PAD_SEG
    recur_y = pl.pallas_call(
        recurrent_kernel,
        out_shape=jax.ShapeDtypeStruct((length, channels), jnp.bfloat16),
        in_specs=[SMEM] + [VMEM] * 15,
        out_specs=VMEM,
        scratch_shapes=[
            pltpu.VMEM((length, D), jnp.bfloat16),
            pltpu.VMEM((D, 256), jnp.bfloat16),
            pltpu.VMEM((channels, 4 * channels), jnp.bfloat16),
            pltpu.VMEM((length + 16, channels), jnp.float32),
            pltpu.VMEM((2, seg_rows, channels), jnp.float32),
            pltpu.VMEM((2, seg_rows, channels), jnp.float32),
            pltpu.VMEM((2, seg_rows, channels), jnp.float32),
        ],
        name="recurrent",
    )(
        where,
        *toks,
        tok_others,
        mixer_gain[None],
        conv_taps,
        recur_gate,
        input_gate,
        coef,
        recur_gain[None],
        *in_y,
    )
    recur = from_all_x(recur_y)
    recur_others = swap_cores(jnp.stack(recur))
    normed, mid_own = pl.pallas_call(
        middle_kernel,
        out_shape=(
            jax.ShapeDtypeStruct((length, D), jnp.bfloat16),
            jax.ShapeDtypeStruct((length, feature_width), jnp.bfloat16),
        ),
        in_specs=[SMEM] + [VMEM] * 17,
        out_specs=(VMEM, VMEM),
        scratch_shapes=[
            pltpu.VMEM((length, 8 * channels), jnp.bfloat16),
            pltpu.VMEM((D, 8 * channels), jnp.bfloat16),
            pltpu.VMEM((length, D), jnp.float32),
        ],
        name="middle",
    )(
        where,
        *toks,
        tok_others,
        *recur,
        recur_others,
        *weights,
        weight_others,
        mixer_post[None],
        channel_gain[None],
    )
    keep, send = pl.pallas_call(
        forward_kernel,
        out_shape=(jax.ShapeDtypeStruct((4, length, 256), jnp.bfloat16),) * 2,
        in_specs=[SMEM] + [VMEM] * 14,
        out_specs=(VMEM, VMEM),
        scratch_shapes=[
            pltpu.VMEM((D, 2 * width), jnp.bfloat16),
            pltpu.VMEM((2, D // 2, width), jnp.bfloat16),
        ],
        name="forward",
    )(where, normed, *hidden_blocks, *down_y)
    came = swap_cores(send)

    def pair(to):
        one = lax.dynamic_index_in_dim(keep, to, 0, False).astype(jnp.float32)
        two = lax.dynamic_index_in_dim(came, to, 0, False).astype(jnp.float32)
        return one + two

    hidden_own = pair(x)
    for k in (1, 2, 3):
        part = shift(pair((x + k) % 4).astype(jnp.bfloat16), "x", k)
        hidden_own = hidden_own + part.astype(jnp.float32)
    energy = jnp.sum(hidden_own * hidden_own, axis=1)
    everyone = jnp.broadcast_to(energy, (8, length))
    energy = jnp.sum(lax.all_to_all(everyone, TP, 0, 0, tiled=True), axis=0)
    post_own = lax.dynamic_slice_in_dim(channel_post, rank_tp * feature_width, feature_width, 0)
    return (
        mid_own.astype(jnp.float32)
        + hidden_own * lax.rsqrt(energy / D + EPS)[:, None] * post_own
    ).astype(jnp.bfloat16)


def solution(mesh):
    split = Mesh(mesh.devices.reshape(8, 4, 4, 2), ("z", "y", "x", "c"))
    placed = (
        P(FS, TP),
        P(),
        P(FS, TP),
        P(FS, TP),
        P(),
        P(),
        P(),
        P(),
        P(),
        P(TP, FS),
        P(),
        P(),
        P(FS, TP),
        P(FS, TP),
        P(TP, FS),
        P(),
    )

    return jax.shard_map(on_device, mesh=split, in_specs=placed, out_specs=P(FS, TP), check_vma=False)
```
